256 devices in a mesh: sp: 16 (over y, x), tp: 16 (over z, core).
Axes of the slice: x: 4, y: 4, z: 8, core: 2. Of those that a mesh axis runs over, the one named last changes fastest.
Arguments:
- query_rows: bfloat16 [65536, 1024], P('sp', 'tp'), may hold values from -6 to 6
- key_rows: bfloat16 [65536, 1024], P('sp', 'tp'), may hold values from -6 to 6
- value_rows: bfloat16 [65536, 1024], P('sp', 'tp'), may hold values from -6 to 6
- gate_rows: bfloat16 [65536, 1024], P('sp', 'tp'), may hold values from -6 to 6
- log_decay: float32 [16, 65536], P('tp', 'sp'), may hold values from -1 to 0
- residual: bfloat16 [65536, 2048], P(('sp', 'tp')), may hold values from -6 to 6
- head_gain: float32 [1024], P('tp'), may hold values from 0.1 to 1.9
- out_weight: bfloat16 [1024, 2048], P(None, 'tp'), may hold values from -0.1875 to 0.1875
- norm_gain: float32 [2048], replicated, may hold values from 0.1 to 1.9
- expert_ids: int32 [65536, 2], P(('sp', 'tp')), may hold values from 0 to 15, all different within a row; in each aligned block of 256 rows (0 to 255, 256 to 511, ...) at most 48 rows name the same one
- route_weights: float32 [65536, 2], P(('sp', 'tp')), may hold values from 0.2 to 1
- expert_gate: bfloat16 [2048, 16384], P(None, ('sp', 'tp')), may hold values from -0.125 to 0.125
- expert_up: bfloat16 [2048, 16384], P(None, ('sp', 'tp')), may hold values from -0.125 to 0.125
- expert_down: bfloat16 [2048, 16384], P(None, ('sp', 'tp')), may hold values from -0.1875 to 0.1875
- shared_gate: bfloat16 [2048, 512], replicated, may hold values from -0.125 to 0.125
- shared_up: bfloat16 [2048, 512], replicated, may hold values from -0.125 to 0.125
- shared_down: bfloat16 [2048, 512], replicated, may hold values from -0.25 to 0.25
Outputs:
- result: bfloat16 [65536, 2048], P(('sp', 'tp'))
The draws below stay inside these ranges and needn't reach their ends.
Inputs may be any that keep to these rules, and one draw needn't show every extreme that they name: `expert_ids`: each row names 2 different experts. Within the rows of one device (aligned blocks of 256 rows) no expert is named by more than 48 rows, and in some block an expert is named by exactly 48 rows.
All inputs are finite; a program needn't handle non-finite values.
Results may differ from the reference program's by a relative error of at most 0.0075.
Values may be sent and summed in bfloat16 or wider, within the bound.
A program may use at most 128 MiB of HBM per device.

```python
import math
import jax
import jax.numpy as jnp
import numpy as np
from jax import lax

D = 2048
HEADS = 16
HEAD = 64
HW = 1024
FF = 1024
SH = 512
TOPK = 2
SPAN = 512
TOK_DEV = 256
TOKENS = 65536
SPECIALISTS = 16
CAP = 48


def draw_log_decay(key, part):
    streams = jax.random.split(key, 6)
    slow_share = 0.5
    sequence_ordinals = jnp.arange(TOKENS, dtype=jnp.int32)
    chance = jax.random.uniform(streams[0], (HEADS,))
    slow = chance < slow_share
    fast_rate = jnp.exp(jax.random.uniform(streams[1], (HEADS,), minval=jnp.log(1.0 / 100.0), maxval=jnp.log(1.0 / 30.0)))
    slow_rate = jnp.exp(jax.random.uniform(streams[2], (HEADS,), minval=jnp.log(0.1), maxval=jnp.log(0.8))) / TOKENS
    rate = jnp.where(slow, slow_rate, fast_rate)
    factor = jnp.exp(jax.random.uniform(streams[3], (16,), minval=jnp.log(0.25), maxval=0.0))
    individual_slot_factor = factor[sequence_ordinals * 16 // TOKENS]
    constant_shrinkage = -rate[:, None] * individual_slot_factor[None, :]
    shifted_locations = jax.random.randint(streams[4], (HEADS, 2), 0, TOKENS)
    stack_level = jax.random.uniform(streams[5], (HEADS, 2), minval=jnp.log(0.5), maxval=jnp.log(0.8))
    segment_bundles = jnp.sum(jnp.where(sequence_ordinals[None, None, :] == shifted_locations[:, :, None], stack_level[:, :, None], 0.0), axis=1)
    return (constant_shrinkage + segment_bundles).astype(jnp.float32)


def block_levels(stream_key, dims, cuts, low, largest):
    gain = 1.0
    for dim, parts in cuts:
        heights = jax.random.uniform(jax.random.fold_in(jax.random.fold_in(stream_key, 6), dim), (parts,), jnp.float32, low / len(cuts), largest / len(cuts))
        gain = gain * jnp.repeat(jnp.exp(heights), dims[dim] // parts).reshape((-1,) + (1,) * (len(dims) - 1 - dim))
    return gain


def deal_out(rng, own, number, rows, count, top, reach, lean):
    sequence = jax.random.permutation(rng, count)
    crowded, common = load_shares(count, rows * top, reach, lean, True), load_shares(count, rows * top, reach, lean, False)
    places = jnp.arange(count)

    def named(lengths, offset_by):
        used = int((lengths > 0).sum())
        fixed = max(1, used // 4)
        moved = fixed + (places - fixed + offset_by * (used - fixed)) % max(1, count - fixed)
        return jnp.zeros((count,), jnp.int32).at[sequence[jnp.where(places < fixed, places, moved)]].set(jnp.asarray(lengths, jnp.int32))

    lengths = jnp.where(number % 4 == 0, named(crowded, number // 4), named(common, number - number // 4 - 1))
    mixed = jax.random.permutation(jax.random.fold_in(own, 3), count)
    giver, sink = mixed[0:count // 2 * 2:2], mixed[1:count // 2 * 2:2]
    slack = jnp.minimum(lengths[giver] - 1, reach - lengths[sink]) // 2
    slack = jnp.where((giver == sequence[0]) | (sink == sequence[0]) | (lengths[sink] == 0), 0, jnp.maximum(slack, 0))
    moved = jax.random.randint(jax.random.fold_in(own, 4), (count // 2,), 0, 1 << 20) % (slack + 1)
    lengths = lengths.at[giver].add(-moved).at[sink].add(moved)
    labels = jnp.searchsorted(jnp.cumsum(lengths), jnp.arange(rows * top), side="right").astype(jnp.int32)
    table = labels.reshape(top, rows).T
    table = table[jax.random.permutation(jax.random.fold_in(own, 1), rows)]
    offset_by = jax.random.randint(jax.random.fold_in(own, 2), (rows, 1), 0, top)
    return jnp.take_along_axis(table, (jnp.arange(top)[None, :] + offset_by) % top, axis=1)


def load_shares(number_of, total, reach, slope, full):
    portions = [(1 << 20) // math.isqrt(standing ** slope) + 1 for standing in range(1, number_of + 1)]
    largest = reach if full else min(reach, max(-(-total // number_of), total * portions[0] // sum(portions)))
    least = 1 if total - largest >= number_of - 1 else 0
    counts, rest = [largest] + [least] * (number_of - 1), total - largest - least * (number_of - 1)
    while rest > 0:
        candidates = [i for i in range(1, number_of) if counts[i] < largest] or [i for i in range(1, number_of) if counts[i] < reach]
        whole, budget = sum([portions[i] for i in candidates]), rest
        for i in candidates:
            addition = min(reach - counts[i], max(1, budget * portions[i] // whole), rest)
            counts[i] = counts[i] + addition
            rest = rest - addition
    return np.array(counts)


def centred(key, dims, scale, limit, pieces=(), kind=jnp.bfloat16):
    loudness = block_levels(key, dims, pieces, -0.22, 0.18) if pieces else 1.0
    array = jax.random.normal(key, dims, jnp.float32) * scale * loudness
    return jnp.minimum(jnp.maximum(array, -limit), limit).astype(kind)


def setup_inputs(seed: int = 0) -> dict:
    streams_of = jax.random.split(jax.random.key(seed), 18)
    query_rows = centred(streams_of[0], (TOKENS, HW), 1.0, 6.0, ((0, 16), (1, 16)))
    key_rows = centred(streams_of[1], (TOKENS, HW), 1.0, 6.0, ((0, 16), (1, 16)))
    value_rows = centred(streams_of[2], (TOKENS, HW), 1.0, 6.0, ((0, 16), (1, 16)))
    gate_rows = centred(streams_of[3], (TOKENS, HW), 1.0, 6.0, ((0, 16), (1, 16)))
    log_decay = draw_log_decay(jax.random.fold_in(streams_of[17], 71), 0)
    residual = centred(streams_of[5], (TOKENS, D), 1.0, 6.0, ((0, 256),))
    head_gain = jnp.clip(1.0 + 0.18 * jax.random.normal(streams_of[6], (HW,), jnp.float32), 0.1, 1.9)
    out_weight = centred(streams_of[7], (HW, D), HW ** -0.5, 0.1875, ((1, 16),))
    norm_gain = jnp.clip(1.0 + 0.18 * jax.random.normal(streams_of[8], (D,), jnp.float32), 0.1, 1.9)
    expert_ids_keys = jax.random.split(jax.random.fold_in(streams_of[9], 1), TOKENS // TOK_DEV)
    expert_ids_turns = jax.random.permutation(jax.random.fold_in(streams_of[9], 3), TOKENS // TOK_DEV)
    expert_ids = jax.vmap(lambda own, number: deal_out(jax.random.fold_in(streams_of[9], 2), own, number, TOK_DEV, SPECIALISTS, TOPK, CAP, 2))(expert_ids_keys, expert_ids_turns).reshape((TOKENS, TOPK))
    route_weights = jnp.clip(jnp.exp(math.log(1.0) - 1.609438 * jax.random.uniform(streams_of[10], (TOKENS, TOPK), jnp.float32) ** block_levels(streams_of[10], (TOKENS, TOPK), ((0, 256),), -0.2, 0.2)), 0.2, 1.0)
    expert_gate = centred(streams_of[11], (D, SPECIALISTS * FF), D ** -0.5, 0.125, ((1, 256),))
    expert_up = centred(streams_of[12], (D, SPECIALISTS * FF), D ** -0.5, 0.125, ((1, 256),))
    expert_down = centred(streams_of[13], (D, SPECIALISTS * FF), FF ** -0.5, 0.1875, ((1, 256),))
    shared_gate = centred(streams_of[14], (D, SH), D ** -0.5, 0.125)
    shared_up = centred(streams_of[15], (D, SH), D ** -0.5, 0.125)
    shared_down = centred(streams_of[16], (D, SH), SH ** -0.5, 0.25)
    return dict(query_rows=query_rows, key_rows=key_rows, value_rows=value_rows, gate_rows=gate_rows, log_decay=log_decay, residual=residual, head_gain=head_gain, out_weight=out_weight, norm_gain=norm_gain, expert_ids=expert_ids, route_weights=route_weights, expert_gate=expert_gate, expert_up=expert_up, expert_down=expert_down, shared_gate=shared_gate, shared_up=shared_up, shared_down=shared_down)


eps = 1e-05

def retain(queries, key_heads, values, log_decay):
    rows, heads, width = queries.shape
    count = rows // SPAN
    scale = width ** (-0.5)
    query_blocks = queries.reshape(count, SPAN, heads, width)
    key_blocks = key_heads.reshape(count, SPAN, heads, width)
    value_blocks = values.reshape(count, SPAN, heads, width)
    decay_blocks = log_decay.reshape(heads, count, SPAN).transpose(1, 0, 2)
    offsets = jnp.arange(SPAN, dtype=jnp.int32)
    causal = offsets[:, None] >= offsets[None, :]

    def advance(carry, inputs):
        block_queries, block_keys, block_values, decay_block = inputs
        query_matrix_full = block_queries.astype(jnp.float32)
        key_matrix_full = block_keys.astype(jnp.float32)
        value_matrix_full = block_values.astype(jnp.float32)
        running = jnp.cumsum(decay_block, axis=1)
        spread = running[:, :, None] - running[:, None, :]
        damping = jnp.exp(jnp.where(causal[None], spread, -jnp.inf))
        attention_scores = jnp.einsum('xru,jru->rxj', query_matrix_full, key_matrix_full)
        decay_weighted = lax.optimization_barrier((attention_scores * scale * damping).astype(jnp.bfloat16)).astype(jnp.float32)
        inner_block_term = jnp.einsum('svc,csj->vsj', decay_weighted, value_matrix_full)
        carried = jnp.einsum('nhd,hde->nhe', query_matrix_full, carry, precision=lax.Precision.HIGHEST)
        carried = carried * jnp.exp(running).T[:, :, None]
        decay_to_block_end = jnp.exp(running[:, -1:] - running).T[:, :, None] * scale
        state_update = jnp.einsum('jok,jow->okw', key_matrix_full * decay_to_block_end, value_matrix_full, precision=lax.Precision.HIGHEST)
        carry = carry * jnp.exp(running[:, -1])[:, None, None] + state_update
        return (carry, inner_block_term + carried)
    start = jnp.zeros((heads, width, width), jnp.float32)
    _, outputs = lax.scan(advance, start, (query_blocks, key_blocks, value_blocks, decay_blocks))
    return outputs.reshape(rows, heads, width)

def reference(query_rows, key_rows, value_rows, gate_rows, log_decay, residual, head_gain, out_weight, norm_gain, expert_ids, route_weights, expert_gate, expert_up, expert_down, shared_gate, shared_up, shared_down):
    retained = retain(query_rows.reshape(TOKENS, HEADS, HEAD), key_rows.reshape(TOKENS, HEADS, HEAD), value_rows.reshape(TOKENS, HEADS, HEAD), log_decay)
    centered = retained - lax.optimization_barrier(jnp.mean(retained, axis=2, keepdims=True))
    normed = centered * lax.rsqrt(lax.optimization_barrier(jnp.mean(centered * centered, axis=2, keepdims=True)) + eps)
    ret_rows = (normed.reshape(TOKENS, HW) * head_gain * jax.nn.silu(gate_rows.astype(jnp.float32))).astype(jnp.bfloat16)
    mixer = jnp.dot(ret_rows, out_weight, preferred_element_type=jnp.float32)
    hidden = (residual.astype(jnp.float32) + mixer).astype(jnp.bfloat16)
    hidden_wide = hidden.astype(jnp.float32)
    normed_rows = (hidden_wide * lax.rsqrt(lax.optimization_barrier(jnp.mean(hidden_wide * hidden_wide, axis=1, keepdims=True)) + eps) * norm_gain).astype(jnp.bfloat16)
    shared_mid = (jax.nn.silu(jnp.dot(normed_rows, shared_gate, preferred_element_type=jnp.float32)) * jnp.dot(normed_rows, shared_up, preferred_element_type=jnp.float32)).astype(jnp.bfloat16)
    shared_out = lax.dot_general(shared_mid, shared_down, (((1,), (1,)), ((), ())), preferred_element_type=jnp.float32)
    block_count = TOKENS // TOK_DEV
    slots = block_count * CAP
    block_index = jnp.arange(block_count, dtype=jnp.int32)[:, None]
    token_index = jnp.arange(TOKENS, dtype=jnp.int32)

    def expert_step(total, index):
        chosen = expert_ids == index
        picked = jnp.any(chosen, axis=1)
        weight = lax.optimization_barrier(jnp.sum(jnp.where(chosen, route_weights, 0.0), axis=1))
        blocked = picked.reshape(block_count, TOK_DEV).astype(jnp.int32)
        position = jnp.cumsum(blocked, axis=1) - 1
        target = jnp.where(blocked > 0, block_index * CAP + position, slots).reshape(-1).astype(jnp.int32)
        table = jnp.zeros((slots + 1,), jnp.int32).at[target].set(token_index)[:slots]
        live = jnp.zeros((slots + 1,), jnp.float32).at[target].set(1.0)[:slots]
        rows = normed_rows[table]
        gate_cols = lax.dynamic_slice_in_dim(expert_gate, index * FF, FF, 1)
        up_cols = lax.dynamic_slice_in_dim(expert_up, index * FF, FF, 1)
        down_cols = lax.dynamic_slice_in_dim(expert_down, index * FF, FF, 1)
        middle = (jax.nn.silu(jnp.dot(rows, gate_cols, preferred_element_type=jnp.float32)) * jnp.dot(rows, up_cols, preferred_element_type=jnp.float32)).astype(jnp.bfloat16)
        outcome = lax.dot_general(middle, down_cols, (((1,), (1,)), ((), ())), preferred_element_type=jnp.float32).astype(jnp.bfloat16)
        contrib = outcome.astype(jnp.float32) * (weight[table] * live)[:, None]
        return (total.at[table].add(contrib), None)
    routed, _ = lax.scan(expert_step, jnp.zeros((TOKENS, D), jnp.float32), jnp.arange(SPECIALISTS, dtype=jnp.int32))
    return (hidden_wide + routed + shared_out).astype(jnp.bfloat16)
```

```python
import jax
import jax.numpy as jnp
from jax import lax
from jax.experimental import pallas as pl
from jax.experimental.pallas import tpu as pltpu
from jax.sharding import PartitionSpec as P

HEAD = 64
BLK = 256
EPS = 1e-05
MESH = pl.DeviceIdType.MESH
F32 = jnp.float32
BF16 = jnp.bfloat16
DEPTH = 3

FAR = [(2, 2), (1, 2), (2, 1), (2, 3), (3, 2), (1, 1), (3, 3), (1, 3), (3, 1), (2, 0), (0, 2), (1, 0), (0, 1), (3, 0), (0, 3)]


def dot(a, b, dims=((1,), (0,))):
    return lax.dot_general(a, b, (dims, ((), ())), preferred_element_type=F32)


def halves(x):
    high = x.astype(BF16)
    return high, (x - high.astype(F32)).astype(BF16)


def layer(
    q_h, k_h, v_h, g_h, ld_ref, res_h, hg_ref, ow_h, ng_ref, ids_ref, rw_ref,
    gate_h, up_h, down_h, sg_h, su_h, sd_h,
    out_ref,
    q, k, v, g, res, gst, ust, dst, sg, su, sd,
    owb, gub, dtb, cs, cb, cl, lp, inn, st, sr, pb, rb, tr, hid, nb,
    xs, xr, yb, yr, mid, acc, wt, smid,
    lsem, ssend, srecv, tsend, trecv, rsend, rrecv, dsend, drecv, xsend, xrecv, ysend, yrecv,
):
    sp, tp = lax.axis_index("sp"), lax.axis_index("tp")
    y, x = sp // 4, sp % 4
    z, c = tp // 2, tp % 2
    sibling = z * 2 + (1 - c)

    def partner(m):
        dy, dx = m
        dy, dx = jnp.where(c == 0, dy, dx), jnp.where(c == 0, dx, dy)
        return ((y + dy) % 4) * 4 + (x + dx) % 4

    partners = [partner(m) for m in FAR]

    def local(i, src, to):
        cp = pltpu.make_async_copy(src, to, lsem.at[i])
        cp.start()
        return cp

    c_ow = local(0, ow_h, owb.at[:, pl.ds(pl.multiple_of(tp * 128, 128), 128)])
    c_k = local(1, k_h, k)
    c_v = local(2, v_h, v)
    c_q = local(3, q_h, q)
    c_gate = local(4, gate_h, gst)
    c_up = local(5, up_h, ust)
    c_down = local(6, down_h, dst)
    c_g = local(7, g_h, g)
    c_res = local(8, res_h, res)
    c_sg = local(9, sg_h, sg)
    c_su = local(10, su_h, su)
    c_sd = local(11, sd_h, sd)

    barrier = pltpu.get_barrier_semaphore()
    for other in partners:
        pl.semaphore_signal(barrier, inc=1, device_id=(other, tp), device_id_type=MESH)
    for step in range(1, 16):
        pl.semaphore_signal(barrier, inc=1, device_id=(sp, (tp + step) % 16), device_id_type=MESH)
    pl.semaphore_wait(barrier, 30)

    def piece(p, j):
        if p < 2:
            return owb.at[pl.ds(512 * p, 512), pl.ds(pl.multiple_of(j * 128, 128), 128)]
        if p < 6:
            return gub.at[j // 2, pl.ds(512 * (p - 2), 512), pl.ds(pl.multiple_of((j % 2) * 128, 128), 128)]
        return dtb.at[pl.ds(pl.multiple_of(j * 64 + 32 * (p - 6), 32), 32), :]

    def hop(way, h, p):
        origin = ((z + 8 - h) % 8 if way == 0 else (z + h) % 8) * 2 + c
        to = ((z + 1) % 8 if way == 0 else (z + 7) % 8) * 2 + c
        ref = piece(p, origin)
        return pltpu.make_async_remote_copy(
            ref, ref, rsend.at[way, h, p], rrecv.at[way, h, p], device_id=(sp, to), device_id_type=MESH
        )

    def arrival(way, h, p):
        origin = ((z + 7 - h) % 8 if way == 0 else (z + h + 1) % 8) * 2 + c
        ref = piece(p, origin)
        return pltpu.make_async_remote_copy(
            ref, ref, rsend.at[way, h, p], rrecv.at[way, h, p], device_id=(sp, sibling), device_id_type=MESH
        )

    def across(o, p, core):
        ref = piece(p, ((z + o) % 8) * 2 + core)
        return pltpu.make_async_remote_copy(
            ref, ref, dsend.at[o, p], drecv.at[o, p], device_id=(sp, sibling), device_id_type=MESH
        )

    flying = {0: [], 1: []}
    crossing = []

    def send(way, h, p):
        if len(flying[way]) >= DEPTH:
            flying[way].pop(0).wait_send()
        cp = hop(way, h, p)
        cp.start()
        flying[way].append(cp)

    def cross(o, p):
        cp = across(o, p, c)
        cp.start()
        crossing.append(cp)

    def event(h, p):
        for way in (0, 1):
            last = p % 2 == way
            if h == 0:
                send(way, 0, p)
                continue
            if h == 4 and not last:
                continue
            arrival(way, h - 1, p).wait_recv()
            if h < 3 or (h == 3 and last):
                send(way, h, p)
            cross((8 - h) % 8 if way == 0 else h, p)
        if h == 0:
            cross(0, p)

    order = [(h, p) for h in range(4) for p in (0, 1)]
    order += [(0, 2), (4, 0), (4, 1), (0, 3), (0, 4), (0, 5), (0, 6), (0, 7)]
    order += [(h, p) for h in (1, 2, 3, 4) for p in range(2, 8)]
    events = iter(order)

    def ring(n):
        for _ in range(n):
            at = next(events, None)
            if at is not None:
                event(*at)

    c_ow.wait()
    ring(2)

    ri = lax.broadcasted_iota(jnp.int32, (BLK, BLK), 0)
    ci = lax.broadcasted_iota(jnp.int32, (BLK, BLK), 1)
    upper = (ri <= ci).astype(F32).astype(BF16)
    lower = (ri >= ci).astype(F32).astype(BF16)
    ld = ld_ref[...]
    d0 = ld.astype(BF16)
    left = ld - d0.astype(F32)
    d1 = left.astype(BF16)
    d2 = (left - d1.astype(F32)).astype(BF16)
    cs[...] = dot(d0, upper) + (dot(d1, upper) + dot(d2, upper))
    nt = ((1,), (1,))
    cols = dot(lower, d0, nt) + (dot(lower, d1, nt) + dot(lower, d2, nt))
    for b in range(16):
        cb[b] = jnp.broadcast_to(cols[:, b : b + 1], (BLK, 128))

    c_k.wait()
    c_v.wait()

    def rows(b):
        return pl.ds(pl.multiple_of(b * BLK, BLK), BLK)

    def state_step(b, carry):
        state, total = carry
        cl[b] = state
        lp[b] = jnp.broadcast_to(total, (8, HEAD))
        end = cb[b, BLK - 1 : BLK, :HEAD]
        kd = k[rows(b), :].astype(F32) * (jnp.exp(end - cb[b, :, :HEAD]) * 0.125)
        high, low = halves(kd)
        vb = v[rows(b), :]
        tn = ((0,), (0,))
        state = state * jnp.exp(end) + (dot(high, vb, tn) + dot(low, vb, tn))
        return state, total + end

    state, total = lax.fori_loop(
        0, 16, state_step, (jnp.zeros((HEAD, HEAD), F32), jnp.zeros((1, HEAD), F32))
    )
    st[...] = jnp.concatenate([state, jnp.broadcast_to(total, (HEAD, HEAD))], axis=1)
    scopies = []
    for i, other in enumerate(partners):
        cp = pltpu.make_async_remote_copy(
            st, sr.at[sp], ssend.at[i], srecv.at[i], device_id=(other, tp), device_id_type=MESH
        )
        cp.start()
        scopies.append(cp)
    sr[sp] = st[...]
    ring(1)
    c_q.wait()

    def inner_step(b, _):
        scores = dot(q[rows(b), :], k[rows(b), :], nt)
        wide = jnp.concatenate([cb[b], cb[b]], axis=1)
        spread = wide - cs[pl.ds(b, 1), :]
        damp = jnp.exp(jnp.where(ri >= ci, spread, -jnp.inf))
        inn[b] = dot((scores * 0.125 * damp).astype(BF16), v[rows(b), :])
        return 0

    for part in range(4):
        lax.fori_loop(part * 4, part * 4 + 4, inner_step, 0)
        ring(1)

    c_gate.wait()
    c_up.wait()
    c_down.wait()
    mine = pl.ds(pl.multiple_of(c * 128, 128), 128)

    def pack_step(i, _):
        at = pl.ds(pl.multiple_of(i * 128, 128), 128)
        gub[z, at, mine] = jnp.concatenate([gst[at, :], ust[at, :]], axis=1)
        dtb[pl.ds(pl.multiple_of(tp * 64, 64), 64), at] = dst[at, :].astype(F32).T.astype(BF16)
        return 0

    lax.fori_loop(0, 16, pack_step, 0)
    ring(1)

    for cp in scopies:
        cp.wait_recv()

    def entering(j, inc):
        have = sr[j]
        return jnp.where(j < sp, inc * jnp.exp(have[:, HEAD:]) + have[:, :HEAD], inc)

    inc = lax.fori_loop(0, 16, entering, jnp.zeros((HEAD, HEAD), F32))
    c_g.wait()

    def gated_step(i, _):
        off = (8 + i) % 16
        b = (tp + off) % 16
        high, low = halves(cl[b] + inc * jnp.exp(lp[b, 0:1, :]))
        qb = q[rows(b), :]
        kept = inn[b] + (dot(qb, high) + dot(qb, low)) * jnp.exp(cb[b, :, :HEAD])
        kept = kept - jnp.mean(kept, axis=1, keepdims=True)
        kept = kept * lax.rsqrt(jnp.mean(kept * kept, axis=1, keepdims=True) + EPS)
        rr = kept * hg_ref[...] * jax.nn.silu(g[rows(b), :].astype(F32))
        pb[b] = jnp.concatenate([rr[:128], rr[128:]], axis=1).astype(BF16)

        @pl.when(off != 0)
        def _():
            pltpu.make_async_remote_copy(
                pb.at[b], rb.at[tp], tsend.at[off], trecv.at[off], device_id=(sp, b), device_id_type=MESH
            ).start()

        @pl.when(off == 0)
        def _():
            rb[tp] = pb[b]

        return 0

    for part in range(4):
        lax.fori_loop(part * 4, part * 4 + 4, gated_step, 0)
        ring(PRE[part])

    e_i = lax.broadcasted_iota(jnp.int32, (16, BLK), 0)
    first, second = ids_ref[0:1, :] == e_i, ids_ref[1:2, :] == e_i
    named = jnp.where(first | second, 1.0, 0.0)
    before = dot(named.astype(BF16), (ri < ci).astype(F32).astype(BF16))
    code = jnp.where(named > 0, before, -1.0)
    share = jnp.where(first, rw_ref[0:1, :], 0.0) + jnp.where(second, rw_ref[1:2, :], 0.0)
    codes = jnp.broadcast_to(code[:, None, :], (16, 16, BLK)).reshape(BLK, BLK)
    shares = jnp.broadcast_to(share[:, None, :], (16, 16, BLK)).reshape(BLK, BLK)
    slot = (ri % 16).astype(F32)
    for j in range(3):
        chosen = codes == slot + 16.0 * j
        wt[j] = jnp.where(chosen, 1.0, 0.0).astype(BF16)
        high, low = halves(jnp.where(chosen, shares, 0.0))
        wt[3 + j] = high
        wt[6 + j] = low

    ring(2)

    for off in range(1, 16):
        pltpu.make_async_remote_copy(
            pb.at[0], rb.at[0], tsend.at[off], trecv.at[off], device_id=(sp, sibling), device_id_type=MESH
        ).wait_recv()
    lane = lax.broadcasted_iota(jnp.int32, (128, 128), 1) < 64
    for i in range(8):
        a, b = rb[2 * i].astype(F32), rb[2 * i + 1].astype(F32)
        tr[0:128, 128 * i : 128 * i + 128] = jnp.where(lane, a, pltpu.roll(b, 64, 1)).astype(BF16)
        tr[128:256, 128 * i : 128 * i + 128] = jnp.where(lane, pltpu.roll(a, 64, 1), b).astype(BF16)

    for o in range(8):
        for p in (0, 1):
            across(o, p, 1 - c).wait_recv()
    c_res.wait()

    def wide(n):
        return pl.ds(pl.multiple_of(n * 256, 256), 256)

    def mixer_step(n, squares):
        h = (res[:, wide(n)].astype(F32) + dot(tr[...], owb[:, wide(n)])).astype(BF16)
        hid[:, wide(n)] = h
        h = h.astype(F32)
        h = h * h
        return squares + h[:, :128] + h[:, 128:]

    squares = lax.fori_loop(0, 8, mixer_step, jnp.zeros((BLK, 128), F32))
    scale = lax.rsqrt(jnp.sum(squares, axis=1, keepdims=True) * (1.0 / 2048.0) + EPS)

    def norm_step(n, _):
        nb[:, wide(n)] = (hid[:, wide(n)].astype(F32) * scale * ng_ref[:, wide(n)]).astype(BF16)
        return 0

    lax.fori_loop(0, 8, norm_step, 0)

    xcopies = []
    for j in range(3):

        def pick_step(n, _):
            xs[j, :, :, wide(n)] = dot(wt[j], nb[:, wide(n)]).astype(BF16).reshape(16, 16, 256)
            return 0

        lax.fori_loop(0, 8, pick_step, 0)
        for i, other in enumerate(partners):
            cp = pltpu.make_async_remote_copy(
                xs.at[j, other], xr.at[j, sp], xsend.at[j, i], xrecv.at[j, i], device_id=(other, tp), device_id_type=MESH
            )
            cp.start()
            xcopies.append(cp)
        xr[j, sp] = xs[j, sp]
        ring(1)

    c_sg.wait()
    c_su.wait()

    def shared_step(n, _):
        a = dot(nb[...], sg[:, wide(n)])
        smid[:, wide(n)] = (jax.nn.silu(a) * dot(nb[...], su[:, wide(n)])).astype(BF16)
        return 0

    lax.fori_loop(0, 2, shared_step, 0)
    ring(1)
    c_sd.wait()

    def shared_out(n, _):
        acc[:, wide(n)] = dot(smid[...], sd[wide(n), :], nt) + hid[:, wide(n)].astype(F32)
        return 0

    lax.fori_loop(0, 8, shared_out, 0)
    ring(100)
    for o in range(8):
        for p in range(2, 8):
            across(o, p, 1 - c).wait_recv()

    lane = lax.broadcasted_iota(jnp.int32, (BLK, 128), 1) < 64
    ycopies = []
    for j in range(3):
        for i in range(15):
            xcopies[j * 15 + i].wait_recv()

        def up_step(n, _):
            h = dot(xr[j].reshape(BLK, 2048), gub[n])
            a, b = h[:, :128], h[:, 128:]
            opened = jnp.where(lane, a, pltpu.roll(b, 64, 1))
            lifted = jnp.where(lane, pltpu.roll(a, 64, 1), b)
            mid[:, pl.ds(pl.multiple_of(n * 128, 128), 128)] = (jax.nn.silu(opened) * lifted).astype(BF16)
            return 0

        lax.fori_loop(0, 8, up_step, 0)

        def down_step(n, _):
            yb[j, :, :, wide(n)] = dot(mid[...], dtb[:, wide(n)]).astype(BF16).reshape(16, 16, 256)
            return 0

        lax.fori_loop(0, 8, down_step, 0)
        for i, other in enumerate(partners):
            cp = pltpu.make_async_remote_copy(
                yb.at[j, other], yr.at[j, sp], ysend.at[j, i], yrecv.at[j, i], device_id=(other, tp), device_id_type=MESH
            )
            cp.start()
            ycopies.append(cp)
        yr[j, sp] = yb[j, sp]

    tn = ((0,), (0,))
    for j in range(3):
        for i in range(15):
            ycopies[j * 15 + i].wait_recv()

        def sum_step(n, _):
            back = yr[j, :, :, wide(n)].reshape(BLK, 256)
            sums = acc[:, wide(n)] + (dot(wt[3 + j], back, tn) + dot(wt[6 + j], back, tn))
            if j < 2:
                acc[:, wide(n)] = sums
            else:
                out_ref[:, wide(n)] = sums.astype(BF16)
            return 0

        lax.fori_loop(0, 8, sum_step, 0)

    for cp in scopies + xcopies + ycopies + crossing + flying[0] + flying[1]:
        cp.wait_send()
    for off in range(1, 16):
        pltpu.make_async_remote_copy(
            pb.at[0], rb.at[0], tsend.at[off], trecv.at[off], device_id=(sp, sibling), device_id_type=MESH
        ).wait_send()


PRE = (1, 0, 0, 0)


def on_device(
    query_rows, key_rows, value_rows, gate_rows, log_decay, residual, head_gain, out_weight, norm_gain,
    expert_ids, route_weights, expert_gate, expert_up, expert_down, shared_gate, shared_up, shared_down,
):
    anywhere = pl.BlockSpec(memory_space=pl.ANY)
    inside = pl.BlockSpec(memory_space=pltpu.VMEM)
    dma = pltpu.SemaphoreType.DMA
    vm = pltpu.VMEM
    return pl.pallas_call(
        layer,
        name="layer",
        out_shape=jax.ShapeDtypeStruct((256, 2048), BF16),
        in_specs=[anywhere] * 4 + [inside, anywhere, inside, anywhere, inside, inside, inside] + [anywhere] * 6,
        out_specs=inside,
        scratch_shapes=[
            *[vm((4096, 64), BF16)] * 4,
            vm((256, 2048), BF16),
            *[vm((2048, 64), BF16)] * 3,
            *[vm((2048, 512), BF16)] * 3,
            vm((1024, 2048), BF16),
            vm((8, 2048, 256), BF16),
            vm((1024, 2048), BF16),
            vm((16, 256), F32),
            vm((16, 256, 128), F32),
            vm((16, 64, 64), F32),
            vm((16, 8, 64), F32),
            vm((16, 256, 64), F32),
            vm((64, 128), F32),
            vm((16, 64, 128), F32),
            vm((16, 128, 128), BF16),
            vm((16, 128, 128), BF16),
            vm((256, 1024), BF16),
            vm((256, 2048), BF16),
            vm((256, 2048), BF16),
            *[vm((3, 16, 16, 2048), BF16)] * 4,
            vm((256, 1024), BF16),
            vm((256, 2048), F32),
            vm((9, 256, 256), BF16),
            vm((256, 512), BF16),
            dma((12,)),
            dma((15,)), dma((15,)),
            dma((16,)), dma((16,)),
            dma((2, 4, 8)), dma((2, 4, 8)),
            dma((8, 8)), dma((8, 8)),
            dma((3, 15)), dma((3, 15)),
            dma((3, 15)), dma((3, 15)),
        ],
        compiler_params=pltpu.CompilerParams(
            collective_id=0, has_side_effects=True, vmem_limit_bytes=63 * 1024 * 1024
        ),
    )(
        query_rows, key_rows, value_rows, gate_rows, log_decay.reshape(16, 256), residual,
        head_gain.reshape(1, 64), out_weight, norm_gain.reshape(1, 2048), expert_ids.T, route_weights.T,
        expert_gate, expert_up, expert_down, shared_gate, shared_up, shared_down,
    )


def solution(mesh):
    placed = (
        P("sp", "tp"),
        P("sp", "tp"),
        P("sp", "tp"),
        P("sp", "tp"),
        P("tp", "sp"),
        P(("sp", "tp"), None),
        P("tp"),
        P(None, "tp"),
        P(),
        P(("sp", "tp"), None),
        P(("sp", "tp"), None),
        P(None, ("sp", "tp")),
        P(None, ("sp", "tp")),
        P(None, ("sp", "tp")),
        P(),
        P(),
        P(),
    )
    return jax.shard_map(
        on_device, mesh=mesh, in_specs=placed, out_specs=P(("sp", "tp"), None), check_vma=False
    )
```

```python
import jax
import jax.numpy as jnp
from jax import lax
from jax.experimental import pallas as pl
from jax.experimental.pallas import tpu as pltpu
from jax.sharding import PartitionSpec as P

HEAD = 64
BLK = 256
EPS = 1e-05
MESH = pl.DeviceIdType.MESH
F32 = jnp.float32
BF16 = jnp.bfloat16
DEPTH = 3

FAR = [(2, 2), (1, 2), (2, 1), (2, 3), (3, 2), (1, 1), (3, 3), (1, 3), (3, 1), (2, 0), (0, 2), (1, 0), (0, 1), (3, 0), (0, 3)]


def dot(a, b, dims=((1,), (0,))):
    return lax.dot_general(a, b, (dims, ((), ())), preferred_element_type=F32)


def halves(x):
    high = x.astype(BF16)
    return high, (x - high.astype(F32)).astype(BF16)


def layer(
    q_h, k_h, v_h, g_h, ld_ref, res_h, hg_ref, ow_h, ng_ref, ids_ref, rw_ref,
    gate_h, up_h, down_h, sg_h, su_h, sd_h,
    out_ref,
    q, k, v, g, res, sg, su, sd, ows, owb, gateb, upb, downb,
    cs, cb, cl, lp, inn, st, sr, pb, rb, tr, hid, nb,
    xs, xr, yb, yr, mid, acc, wt, smid,
    lsem, ssend, srecv, tsend, trecv, osend, orecv, wsend, wrecv, vsend, vrecv,
    rsend, rrecv, dsend, drecv, xsend, xrecv, ysend, yrecv,
):
    sp, tp = lax.axis_index("sp"), lax.axis_index("tp")
    y, x = sp // 4, sp % 4
    z, c = tp // 2, tp % 2
    sibling = z * 2 + (1 - c)
    nt, tn = ((1,), (1,)), ((0,), (0,))

    def partner(m):
        dy, dx = m
        dy, dx = jnp.where(c == 0, dy, dx), jnp.where(c == 0, dx, dy)
        return ((y + dy) % 4) * 4 + (x + dx) % 4

    partners = [partner(m) for m in FAR]

    def remote(src, to, here, there, device):
        return pltpu.make_async_remote_copy(src, to, here, there, device_id=device, device_id_type=MESH)

    def local(i, src, to):
        cp = pltpu.make_async_copy(src, to, lsem.at[i])
        cp.start()
        return cp

    def block(ref, size, i):
        return ref.at[pl.ds(pl.multiple_of(i * size, size), size)]

    c_ow = local(0, ow_h, ows)
    c_gate = local(1, gate_h, block(gateb, 64, tp))
    c_up = local(2, up_h, block(upb, 64, tp))
    c_down = local(3, down_h, block(downb, 64, tp))
    c_k = local(4, k_h, k)
    c_v = local(5, v_h, v)
    c_q = local(6, q_h, q)
    c_g = local(7, g_h, g)
    c_res = local(8, res_h, res)
    c_sg = local(9, sg_h, sg)
    c_su = local(10, su_h, su)
    c_sd = local(11, sd_h, sd)

    barrier = pltpu.get_barrier_semaphore()
    for other in partners:
        pl.semaphore_signal(barrier, inc=1, device_id=(other, tp), device_id_type=MESH)
    for step in range(1, 16):
        pl.semaphore_signal(barrier, inc=1, device_id=(sp, (tp + step) % 16), device_id_type=MESH)
    pl.semaphore_wait(barrier, 30)

    def piece(p, j):
        ref = (gateb, upb, downb)[p // 2]
        return ref.at[pl.ds(pl.multiple_of(j * 64 + 32 * (p % 2), 32), 32)]

    def hop(way, h, p):
        origin = ((z + 8 - h) % 8 if way == 0 else (z + h) % 8) * 2 + c
        to = ((z + 1) % 8 if way == 0 else (z + 7) % 8) * 2 + c
        ref = piece(p, origin)
        return remote(ref, ref, rsend.at[way, h, p], rrecv.at[way, h, p], (sp, to))

    def arrival(way, h, p):
        origin = ((z + 7 - h) % 8 if way == 0 else (z + h + 1) % 8) * 2 + c
        ref = piece(p, origin)
        return remote(ref, ref, rsend.at[way, h, p], rrecv.at[way, h, p], (sp, sibling))

    def across(o, p, core):
        ref = piece(p, ((z + o) % 8) * 2 + core)
        return remote(ref, ref, dsend.at[o, p], drecv.at[o, p], (sp, sibling))

    flying = {0: [], 1: []}
    started = []

    def go(cp):
        cp.start()
        started.append(cp)
        return cp

    def send(way, h, p):
        if len(flying[way]) >= DEPTH:
            flying[way].pop(0).wait_send()
        cp = hop(way, h, p)
        cp.start()
        flying[way].append(cp)

    def event(h, p):
        for way in (0, 1):
            last = p % 2 == way
            if h == 0:
                send(way, 0, p)
                continue
            if h == 4 and not last:
                continue
            arrival(way, h - 1, p).wait_recv()
            if h < 3 or (h == 3 and last):
                send(way, h, p)
            go(across((8 - h) % 8 if way == 0 else h, p, c))
        if h == 0:
            go(across(0, p, c))

    events = [(h, p) for h in range(5) for p in range(6)]

    def ring(n):
        for _ in range(n):
            if events:
                event(*events.pop(0))

    def slice_of(core):
        return pl.ds(pl.multiple_of(sp * 64 + core * 32, 32), 32)

    def columns_of(j):
        return pl.ds(pl.multiple_of(j * 128, 128), 128)

    c_ow.wait()
    for step in range(1, 16):
        other = (tp + step) % 16
        go(remote(
            ows.at[slice_of((c + step) % 2), :], owb.at[slice_of((c + step) % 2), columns_of(tp)],
            osend.at[step], orecv.at[step], (sp, other),
        ))
    owb[slice_of(c), columns_of(tp)] = ows[slice_of(c), :]
    c_gate.wait()
    c_up.wait()
    c_down.wait()
    ring(FIRST)

    ri = lax.broadcasted_iota(jnp.int32, (BLK, BLK), 0)
    ci = lax.broadcasted_iota(jnp.int32, (BLK, BLK), 1)
    upper = (ri <= ci).astype(F32).astype(BF16)
    lower = (ri >= ci).astype(F32).astype(BF16)
    for b in range(16):
        cs[b : b + 1, :] = ld_ref[0:1, b * BLK : b * BLK + BLK]
    ld = cs[...]
    d0 = ld.astype(BF16)
    left = ld - d0.astype(F32)
    d1 = left.astype(BF16)
    d2 = (left - d1.astype(F32)).astype(BF16)
    cs[...] = dot(d0, upper) + (dot(d1, upper) + dot(d2, upper))
    cols = dot(lower, d0, nt) + (dot(lower, d1, nt) + dot(lower, d2, nt))
    for b in range(16):
        cb[b] = jnp.broadcast_to(cols[:, b : b + 1], (BLK, 128))

    c_k.wait()
    c_v.wait()

    def at(b):
        return pl.ds(pl.multiple_of(b * BLK, BLK), BLK)

    def state_step(b, carry):
        state, total = carry
        cl[b] = state
        lp[b] = jnp.broadcast_to(total, (8, 128))
        end = cb[b, BLK - 1 : BLK, :]
        wide = jnp.concatenate([end, end], axis=1)
        kd = k[:, at(b)].astype(F32) * (jnp.exp(wide - cs[pl.ds(b, 1), :]) * 0.125)
        high, low = halves(kd)
        vb = v[:, at(b)]
        state = state * jnp.exp(end[:, :HEAD]) + (dot(vb, high, nt) + dot(vb, low, nt))
        return state, total + end

    state, total = lax.fori_loop(
        0, 16, state_step, (jnp.zeros((HEAD, HEAD), F32), jnp.zeros((1, 128), F32)), unroll=2
    )
    st[0:32] = jnp.concatenate([state[:32], state[32:]], axis=1)
    st[32:40] = jnp.broadcast_to(total, (8, 128))
    scopies = []
    for i, other in enumerate(partners):
        scopies.append(go(remote(st, sr.at[sp], ssend.at[i], srecv.at[i], (other, tp))))
    sr[sp] = st[...]

    for step in range(1, 16):
        remote(
            ows.at[slice_of(c), :], owb.at[slice_of(c), columns_of(tp)], osend.at[step], orecv.at[step], (sp, sibling)
        ).wait_recv()

    def rows_of(s, core):
        return owb.at[pl.ds(pl.multiple_of(s * 64 + core * 32, 32), 32)]

    wcopies = []
    for i, other in enumerate(partners):
        wcopies.append(go(remote(rows_of(sp, c), rows_of(sp, c), wsend.at[i], wrecv.at[i], (other, tp))))
    go(remote(rows_of(sp, c), rows_of(sp, c), vsend.at[15], vrecv.at[15], (sp, sibling)))
    ring(1)
    c_q.wait()

    def inner_step(b, _):
        scores = dot(k[:, at(b)], q[:, at(b)], tn)
        spread = cs[pl.ds(b, 1), :] - jnp.concatenate([cb[b], cb[b]], axis=1)
        damp = jnp.exp(jnp.where(ri <= ci, spread, -jnp.inf))
        inn[b] = dot(v[:, at(b)], (scores * 0.125 * damp).astype(BF16))
        return 0

    for part in range(2):
        lax.fori_loop(part * 8, part * 8 + 8, inner_step, 0, unroll=2)
        ring(1)

    e_i = lax.broadcasted_iota(jnp.int32, (16, BLK), 0)
    first, second = ids_ref[0:1, :] == e_i, ids_ref[1:2, :] == e_i
    named = jnp.where(first | second, 1.0, 0.0)
    before = dot(named.astype(BF16), (ri < ci).astype(F32).astype(BF16))
    code = jnp.where(named > 0, before, -1.0)
    share = jnp.where(first, rw_ref[0:1, :], 0.0) + jnp.where(second, rw_ref[1:2, :], 0.0)
    codes = jnp.broadcast_to(code[:, None, :], (16, 16, BLK)).reshape(BLK, BLK)
    shares = jnp.broadcast_to(share[:, None, :], (16, 16, BLK)).reshape(BLK, BLK)
    slot = (ri % 16).astype(F32)
    for j in range(3):
        chosen = codes == slot + 16.0 * j
        wt[j] = jnp.where(chosen, 1.0, 0.0).astype(BF16)
        high, low = halves(jnp.where(chosen, shares, 0.0).T)
        wt[3 + j] = high
        wt[6 + j] = low

    gain = jnp.broadcast_to(hg_ref[...], (BLK, HEAD)).T
    c_g.wait()
    for cp in scopies:
        cp.wait_recv()

    def entering(j, inc):
        have = sr[j]
        return jnp.where(j < sp, inc * jnp.exp(have[32:33]) + have[:32], inc)

    packed = lax.fori_loop(0, 16, entering, jnp.zeros((32, 128), F32))
    inc = jnp.concatenate([packed[:, :HEAD], packed[:, HEAD:]], axis=0)

    def gated(i):
        off = (8 + i) % 16
        b = (tp + off) % 16
        high, low = halves(cl[b] + inc * jnp.exp(lp[b, 0:1, :HEAD]))
        qb = q[:, at(b)]
        kept = inn[b] + (dot(high, qb) + dot(low, qb)) * jnp.exp(cs[pl.ds(b, 1), :])
        kept = kept - jnp.mean(kept, axis=0, keepdims=True)
        kept = kept * lax.rsqrt(jnp.mean(kept * kept, axis=0, keepdims=True) + EPS)
        pb[b] = (kept * gain * jax.nn.silu(g[:, at(b)].astype(F32))).astype(BF16)
        return off, b

    def gated_step(i, _):
        pairs = [gated(2 * i), gated(2 * i + 1)]
        for off, b in pairs:

            @pl.when(off != 0)
            def _():
                remote(pb.at[b], rb.at[tp], tsend.at[off], trecv.at[off], (sp, b)).start()

            @pl.when(off == 0)
            def _():
                rb[tp] = pb[b]

        return 0

    lax.fori_loop(0, 8, gated_step, 0)
    ring(AFTER_GATED)

    for i, other in enumerate(partners):
        dy, dx = FAR[i]
        origin = partner(((4 - dy) % 4, (4 - dx) % 4))
        wcopies[i].wait_recv()
        go(remote(rows_of(origin, c), rows_of(origin, c), vsend.at[i], vrecv.at[i], (sp, sibling)))

    for off in range(1, 16):
        remote(pb.at[0], rb.at[0], tsend.at[off], trecv.at[off], (sp, sibling)).wait_recv()
    for i in range(8):
        both = jnp.concatenate([rb[2 * i], rb[2 * i + 1]], axis=0)
        tr[:, 128 * i : 128 * i + 128] = both.astype(F32).T.astype(BF16)
    ring(1)
    for i in range(16):
        remote(rows_of(sp, c), rows_of(sp, c), vsend.at[i], vrecv.at[i], (sp, sibling)).wait_recv()
    c_res.wait()

    def wide(n):
        return pl.ds(pl.multiple_of(n * 256, 256), 256)

    def mixer_step(n, squares):
        h = (res[:, wide(n)].astype(F32) + dot(tr[...], owb[:, wide(n)])).astype(BF16)
        hid[:, wide(n)] = h
        h = h.astype(F32)
        h = h * h
        return squares + h[:, :128] + h[:, 128:]

    squares = lax.fori_loop(0, 8, mixer_step, jnp.zeros((BLK, 128), F32))
    scale = lax.rsqrt(jnp.sum(squares, axis=1, keepdims=True) * (1.0 / 2048.0) + EPS)
    ring(1)

    def norm_step(n, _):
        nb[:, wide(n)] = (hid[:, wide(n)].astype(F32) * scale * ng_ref[:, wide(n)]).astype(BF16)
        return 0

    lax.fori_loop(0, 8, norm_step, 0)

    xcopies = []
    for j in range(3):

        def pick_step(n, _):
            xs[j, :, :, wide(n)] = dot(wt[j], nb[:, wide(n)]).astype(BF16).reshape(16, 16, 256)
            return 0

        lax.fori_loop(0, 8, pick_step, 0)
        for i, other in enumerate(partners):
            xcopies.append(go(remote(xs.at[j, other], xr.at[j, sp], xsend.at[j, i], xrecv.at[j, i], (other, tp))))
        xr[j, sp] = xs[j, sp]
        ring(1)

    c_sg.wait()
    c_su.wait()

    def shared_step(n, _):
        a = dot(nb[...], sg[:, wide(n)])
        smid[:, wide(n)] = (jax.nn.silu(a) * dot(nb[...], su[:, wide(n)])).astype(BF16)
        return 0

    lax.fori_loop(0, 2, shared_step, 0)
    ring(1)
    c_sd.wait()

    def shared_out(n, _):
        acc[:, wide(n)] = dot(smid[...], sd[wide(n), :], nt) + hid[:, wide(n)].astype(F32)
        return 0

    lax.fori_loop(0, 8, shared_out, 0)
    ring(len(events) - 12)

    def opened(j, n):
        at_n = pl.ds(pl.multiple_of(n * 128, 128), 128)
        rows = xr[j].reshape(BLK, 2048)
        h = dot(rows, jnp.concatenate([gateb[at_n, :], upb[at_n, :]], axis=0), nt)
        mid[:, at_n] = (jax.nn.silu(h[:, :128]) * h[:, 128:]).astype(BF16)

    def landed(offsets, pieces):
        for o in offsets:
            for p in pieces:
                across(o, p, 1 - c).wait_recv()

    for i in range(15):
        xcopies[i].wait_recv()

    def near(i, _):
        opened(0, (z + i + 6) % 8)
        return 0

    def third(i, _):
        opened(0, (z + 3 + 2 * i) % 8)
        return 0

    landed((0, 1, 2, 6, 7), range(4))
    lax.fori_loop(0, 5, near, 0)
    ring(6)
    landed((3, 5), range(4))
    lax.fori_loop(0, 2, third, 0)
    ring(4)
    landed((4,), range(4))
    opened(0, (z + 4) % 8)
    ring(2)
    landed(range(8), (4, 5))

    ycopies = []
    for j in range(3):
        if j > 0:
            for i in range(15):
                xcopies[j * 15 + i].wait_recv()

            def up_step(n, _):
                opened(j, n)
                return 0

            lax.fori_loop(0, 8, up_step, 0)

        def down_step(n, _):
            yb[j, :, :, wide(n)] = dot(mid[...], downb[:, wide(n)]).astype(BF16).reshape(16, 16, 256)
            return 0

        lax.fori_loop(0, 8, down_step, 0)
        for i, other in enumerate(partners):
            ycopies.append(go(remote(yb.at[j, other], yr.at[j, sp], ysend.at[j, i], yrecv.at[j, i], (other, tp))))
        yr[j, sp] = yb[j, sp]

    for j in range(3):
        for i in range(15):
            ycopies[j * 15 + i].wait_recv()

        def sum_step(n, _):
            back = yr[j, :, :, wide(n)].reshape(BLK, 256)
            sums = acc[:, wide(n)] + (dot(wt[3 + j], back) + dot(wt[6 + j], back))
            if j < 2:
                acc[:, wide(n)] = sums
            else:
                out_ref[:, wide(n)] = sums.astype(BF16)
            return 0

        lax.fori_loop(0, 8, sum_step, 0)

    for cp in started + flying[0] + flying[1]:
        cp.wait_send()
    for off in range(1, 16):
        remote(pb.at[0], rb.at[0], tsend.at[off], trecv.at[off], (sp, sibling)).wait_send()


FIRST = 3
AFTER_GATED = 2


def on_device(
    query_rows, key_rows, value_rows, gate_rows, log_decay, residual, head_gain, out_weight, norm_gain,
    expert_ids, route_weights, expert_gate, expert_up, expert_down, shared_gate, shared_up, shared_down,
):
    anywhere = pl.BlockSpec(memory_space=pl.ANY)
    inside = pl.BlockSpec(memory_space=pltpu.VMEM)
    dma = pltpu.SemaphoreType.DMA
    vm = pltpu.VMEM
    return pl.pallas_call(
        layer,
        name="layer",
        out_shape=jax.ShapeDtypeStruct((256, 2048), BF16),
        in_specs=[anywhere] * 4 + [inside, anywhere, inside, anywhere, inside, inside, inside] + [anywhere] * 6,
        out_specs=inside,
        scratch_shapes=[
            *[vm((64, 4096), BF16)] * 4,
            vm((256, 2048), BF16),
            *[vm((2048, 512), BF16)] * 3,
            vm((1024, 128), BF16),
            *[vm((1024, 2048), BF16)] * 4,
            vm((16, 256), F32),
            vm((16, 256, 128), F32),
            vm((16, 64, 64), F32),
            vm((16, 8, 128), F32),
            vm((16, 64, 256), F32),
            vm((40, 128), F32),
            vm((16, 40, 128), F32),
            vm((16, 64, 256), BF16),
            vm((16, 64, 256), BF16),
            vm((256, 1024), BF16),
            vm((256, 2048), BF16),
            vm((256, 2048), BF16),
            *[vm((3, 16, 16, 2048), BF16)] * 4,
            vm((256, 1024), BF16),
            vm((256, 2048), F32),
            vm((9, 256, 256), BF16),
            vm((256, 512), BF16),
            dma((12,)),
            dma((15,)), dma((15,)),
            dma((16,)), dma((16,)),
            dma((16,)), dma((16,)),
            dma((15,)), dma((15,)),
            dma((16,)), dma((16,)),
            dma((2, 4, 6)), dma((2, 4, 6)),
            dma((8, 6)), dma((8, 6)),
            dma((3, 15)), dma((3, 15)),
            dma((3, 15)), dma((3, 15)),
        ],
        compiler_params=pltpu.CompilerParams(
            collective_id=0, has_side_effects=True, vmem_limit_bytes=63 * 1024 * 1024
        ),
    )(
        query_rows.T, key_rows.T, value_rows.T, gate_rows.T, log_decay, residual,
        head_gain.reshape(1, 64), out_weight, norm_gain.reshape(1, 2048), expert_ids.T, route_weights.T,
        expert_gate.T, expert_up.T, expert_down.T, shared_gate, shared_up, shared_down,
    )


def solution(mesh):
    placed = (
        P("sp", "tp"),
        P("sp", "tp"),
        P("sp", "tp"),
        P("sp", "tp"),
        P("tp", "sp"),
        P(("sp", "tp"), None),
        P("tp"),
        P(None, "tp"),
        P(),
        P(("sp", "tp"), None),
        P(("sp", "tp"), None),
        P(None, ("sp", "tp")),
        P(None, ("sp", "tp")),
        P(None, ("sp", "tp")),
        P(),
        P(),
        P(),
    )
    return jax.shard_map(
        on_device, mesh=mesh, in_specs=placed, out_specs=P(("sp", "tp"), None), check_vma=False
    )
```

```python
import jax
import jax.numpy as jnp
from jax import lax
from jax.experimental import pallas as pl
from jax.experimental.pallas import tpu as pltpu
from jax.sharding import PartitionSpec as P

HEAD = 64
BLK = 256
EPS = 1e-05
MESH = pl.DeviceIdType.MESH
F32 = jnp.float32
BF16 = jnp.bfloat16
DEPTH = 3
PARTS = 2

FAR = [(2, 2), (1, 2), (2, 1), (2, 3), (3, 2), (1, 1), (3, 3), (1, 3), (3, 1), (2, 0), (0, 2), (1, 0), (0, 1), (3, 0), (0, 3)]


def dot(a, b, dims=((1,), (0,))):
    return lax.dot_general(a, b, (dims, ((), ())), preferred_element_type=F32)


def halves(x):
    high = x.astype(BF16)
    return high, (x - high.astype(F32)).astype(BF16)


def layer(
    q_h, k_h, v_h, g_h, ld_ref, res_h, hg_ref, ow_h, ng_ref, ids_ref, rw_ref,
    gate_h, up_h, down_h, sg_h, su_h, sd_h,
    out_ref,
    q, k, v, g, res, sg, su, sd, ows, owb, gateb, upb, downb,
    cs, cb, cl, lp, inn, st, sr, pb, rb, tr, hid, nb,
    xs, xr, yb, yr, mid, acc, wt, smid,
    lsem, ssend, srecv, tsend, trecv, osend, orecv, wsend, wrecv, vsend, vrecv,
    rsend, rrecv, dsend, drecv, xsend, xrecv, ysend, yrecv,
):
    sp, tp = lax.axis_index("sp"), lax.axis_index("tp")
    y, x = sp // 4, sp % 4
    z, c = tp // 2, tp % 2
    sibling = z * 2 + (1 - c)
    nt, tn = ((1,), (1,)), ((0,), (0,))

    def partner(m):
        dy, dx = m
        dy, dx = jnp.where(c == 0, dy, dx), jnp.where(c == 0, dx, dy)
        return ((y + dy) % 4) * 4 + (x + dx) % 4

    partners = [partner(m) for m in FAR]

    def remote(src, to, here, there, device):
        return pltpu.make_async_remote_copy(src, to, here, there, device_id=device, device_id_type=MESH)

    def local(i, src, to):
        cp = pltpu.make_async_copy(src, to, lsem.at[i])
        cp.start()
        return cp

    def block(ref, size, i):
        return ref.at[pl.ds(pl.multiple_of(i * size, size), size)]

    c_ow = local(0, ow_h, ows)
    c_gate = local(1, gate_h, block(gateb, 64, tp))
    c_up = local(2, up_h, block(upb, 64, tp))
    c_down = local(3, down_h, block(downb, 64, tp))
    c_k = local(4, k_h, k)
    c_v = local(5, v_h, v)
    c_q = local(6, q_h, q)
    c_g = local(7, g_h, g)
    c_res = local(8, res_h, res)
    c_sg = local(9, sg_h, sg)
    c_su = local(10, su_h, su)
    c_sd = local(11, sd_h, sd)

    barrier = pltpu.get_barrier_semaphore()
    for other in partners:
        pl.semaphore_signal(barrier, inc=1, device_id=(other, tp), device_id_type=MESH)
    for step in range(1, 16):
        pl.semaphore_signal(barrier, inc=1, device_id=(sp, (tp + step) % 16), device_id_type=MESH)
    pl.semaphore_wait(barrier, 30)

    def piece(p, j):
        ref = (gateb, upb, downb)[p // 2]
        return ref.at[pl.ds(pl.multiple_of(j * 64 + 32 * (p % 2), 32), 32)]

    def hop(way, h, p):
        origin = ((z + 8 - h) % 8 if way == 0 else (z + h) % 8) * 2 + c
        to = ((z + 1) % 8 if way == 0 else (z + 7) % 8) * 2 + c
        ref = piece(p, origin)
        return remote(ref, ref, rsend.at[way, h, p], rrecv.at[way, h, p], (sp, to))

    def arrival(way, h, p):
        origin = ((z + 7 - h) % 8 if way == 0 else (z + h + 1) % 8) * 2 + c
        ref = piece(p, origin)
        return remote(ref, ref, rsend.at[way, h, p], rrecv.at[way, h, p], (sp, sibling))

    def across(o, p, core):
        ref = piece(p, ((z + o) % 8) * 2 + core)
        return remote(ref, ref, dsend.at[o, p], drecv.at[o, p], (sp, sibling))

    flying = {0: [], 1: []}
    started = []

    def go(cp):
        cp.start()
        started.append(cp)
        return cp

    def send(way, h, p):
        if len(flying[way]) >= DEPTH:
            flying[way].pop(0).wait_send()
        cp = hop(way, h, p)
        cp.start()
        flying[way].append(cp)

    def event(h, p):
        for way in (0, 1):
            last = p % 2 == way
            if h == 0:
                send(way, 0, p)
                continue
            if h == 4 and not last:
                continue
            arrival(way, h - 1, p).wait_recv()
            if h < 3 or (h == 3 and last):
                send(way, h, p)
            go(across((8 - h) % 8 if way == 0 else h, p, c))
        if h == 0:
            go(across(0, p, c))

    events = [(h, p) for h in range(5) for p in range(6)]

    def ring(n):
        for _ in range(n):
            if events:
                event(*events.pop(0))

    def slice_of(core):
        return pl.ds(pl.multiple_of(sp * 64 + core * 32, 32), 32)

    def columns_of(j):
        return pl.ds(pl.multiple_of(j * 128, 128), 128)

    c_ow.wait()
    for step in range(1, 16):
        other = (tp + step) % 16
        go(remote(
            ows.at[slice_of((c + step) % 2), :], owb.at[slice_of((c + step) % 2), columns_of(tp)],
            osend.at[step], orecv.at[step], (sp, other),
        ))
    owb[slice_of(c), columns_of(tp)] = ows[slice_of(c), :]
    c_gate.wait()
    c_up.wait()
    c_down.wait()
    ring(FIRST)

    ri = lax.broadcasted_iota(jnp.int32, (BLK, BLK), 0)
    ci = lax.broadcasted_iota(jnp.int32, (BLK, BLK), 1)
    upper = (ri <= ci).astype(F32).astype(BF16)
    lower = (ri >= ci).astype(F32).astype(BF16)
    for b in range(16):
        cs[b : b + 1, :] = ld_ref[0:1, b * BLK : b * BLK + BLK]
    ld = cs[...]
    d0 = ld.astype(BF16)
    left = ld - d0.astype(F32)
    d1 = left.astype(BF16)
    d2 = (left - d1.astype(F32)).astype(BF16)
    cs[...] = dot(d0, upper) + (dot(d1, upper) + dot(d2, upper))
    cols = dot(lower, d0, nt) + (dot(lower, d1, nt) + dot(lower, d2, nt))
    for b in range(16):
        cb[b] = jnp.broadcast_to(cols[:, b : b + 1], (BLK, 128))

    c_k.wait()
    c_v.wait()

    def at(b):
        return pl.ds(pl.multiple_of(b * BLK, BLK), BLK)

    def state_step(b, carry):
        state, total = carry
        cl[b] = state
        lp[b] = jnp.broadcast_to(total, (8, 128))
        end = cb[b, BLK - 1 : BLK, :]
        wide = jnp.concatenate([end, end], axis=1)
        kd = k[:, at(b)].astype(F32) * (jnp.exp(wide - cs[pl.ds(b, 1), :]) * 0.125)
        high, low = halves(kd)
        vb = v[:, at(b)]
        state = state * jnp.exp(end[:, :HEAD]) + (dot(vb, high, nt) + dot(vb, low, nt))
        return state, total + end

    state, total = lax.fori_loop(
        0, 16, state_step, (jnp.zeros((HEAD, HEAD), F32), jnp.zeros((1, 128), F32)), unroll=2
    )
    st[0:32] = jnp.concatenate([state[:32], state[32:]], axis=1)
    st[32:40] = jnp.broadcast_to(total, (8, 128))
    scopies = []
    for i, other in enumerate(partners):
        scopies.append(go(remote(st, sr.at[sp], ssend.at[i], srecv.at[i], (other, tp))))
    sr[sp] = st[...]

    for step in range(1, 16):
        remote(
            ows.at[slice_of(c), :], owb.at[slice_of(c), columns_of(tp)], osend.at[step], orecv.at[step], (sp, sibling)
        ).wait_recv()

    def rows_of(s, core):
        return owb.at[pl.ds(pl.multiple_of(s * 64 + core * 32, 32), 32)]

    wcopies = []
    for i, other in enumerate(partners):
        wcopies.append(go(remote(rows_of(sp, c), rows_of(sp, c), wsend.at[i], wrecv.at[i], (other, tp))))
    go(remote(rows_of(sp, c), rows_of(sp, c), vsend.at[15], vrecv.at[15], (sp, sibling)))
    ring(1)
    c_q.wait()

    def inner_step(b, _):
        scores = dot(k[:, at(b)], q[:, at(b)], tn)
        spread = cs[pl.ds(b, 1), :] - jnp.concatenate([cb[b], cb[b]], axis=1)
        damp = jnp.exp(jnp.where(ri <= ci, spread, -jnp.inf))
        inn[b] = dot(v[:, at(b)], (scores * 0.125 * damp).astype(BF16))
        return 0

    for part in range(2):
        lax.fori_loop(part * 8, part * 8 + 8, inner_step, 0, unroll=2)
        ring(1)

    e_i = lax.broadcasted_iota(jnp.int32, (16, BLK), 0)
    first, second = ids_ref[0:1, :] == e_i, ids_ref[1:2, :] == e_i
    named = jnp.where(first | second, 1.0, 0.0)
    before = dot(named.astype(BF16), (ri < ci).astype(F32).astype(BF16))
    code = jnp.where(named > 0, before, -1.0)
    share = jnp.where(first, rw_ref[0:1, :], 0.0) + jnp.where(second, rw_ref[1:2, :], 0.0)
    codes = jnp.broadcast_to(code[:, None, :], (16, 16, BLK)).reshape(BLK, BLK)
    shares = jnp.broadcast_to(share[:, None, :], (16, 16, BLK)).reshape(BLK, BLK)
    slot = (ri % 16).astype(F32)
    for j in range(3):
        chosen = codes == slot + 16.0 * j
        wt[j] = jnp.where(chosen, 1.0, 0.0).astype(BF16)
        high, low = halves(jnp.where(chosen, shares, 0.0).T)
        wt[3 + j] = high
        wt[6 + j] = low

    gain = jnp.broadcast_to(hg_ref[...], (BLK, HEAD)).T
    c_g.wait()
    for cp in scopies:
        cp.wait_recv()

    def entering(j, inc):
        have = sr[j]
        return jnp.where(j < sp, inc * jnp.exp(have[32:33]) + have[:32], inc)

    packed = lax.fori_loop(0, 16, entering, jnp.zeros((32, 128), F32))
    inc = jnp.concatenate([packed[:, :HEAD], packed[:, HEAD:]], axis=0)

    def gated(i):
        off = (8 + i) % 16
        b = (tp + off) % 16
        high, low = halves(cl[b] + inc * jnp.exp(lp[b, 0:1, :HEAD]))
        qb = q[:, at(b)]
        kept = inn[b] + (dot(high, qb) + dot(low, qb)) * jnp.exp(cs[pl.ds(b, 1), :])
        kept = kept - jnp.mean(kept, axis=0, keepdims=True)
        kept = kept * lax.rsqrt(jnp.mean(kept * kept, axis=0, keepdims=True) + EPS)
        pb[b] = (kept * gain * jax.nn.silu(g[:, at(b)].astype(F32))).astype(BF16)
        return off, b

    def gated_step(i, _):
        pairs = [gated(2 * i), gated(2 * i + 1)]
        for off, b in pairs:

            @pl.when(off != 0)
            def _():
                remote(pb.at[b], rb.at[tp], tsend.at[off], trecv.at[off], (sp, b)).start()

            @pl.when(off == 0)
            def _():
                rb[tp] = pb[b]

        return 0

    lax.fori_loop(0, 8, gated_step, 0)
    ring(AFTER_GATED)

    for i, other in enumerate(partners):
        dy, dx = FAR[i]
        origin = partner(((4 - dy) % 4, (4 - dx) % 4))
        wcopies[i].wait_recv()
        go(remote(rows_of(origin, c), rows_of(origin, c), vsend.at[i], vrecv.at[i], (sp, sibling)))

    for off in range(1, 16):
        remote(pb.at[0], rb.at[0], tsend.at[off], trecv.at[off], (sp, sibling)).wait_recv()
    for i in range(8):
        both = jnp.concatenate([rb[2 * i], rb[2 * i + 1]], axis=0)
        tr[:, 128 * i : 128 * i + 128] = both.astype(F32).T.astype(BF16)
    ring(1)
    for i in range(16):
        remote(rows_of(sp, c), rows_of(sp, c), vsend.at[i], vrecv.at[i], (sp, sibling)).wait_recv()
    c_res.wait()

    def wide(n):
        return pl.ds(pl.multiple_of(n * 256, 256), 256)

    def mixer_step(n, squares):
        h = (res[:, wide(n)].astype(F32) + dot(tr[...], owb[:, wide(n)])).astype(BF16)
        hid[:, wide(n)] = h
        h = h.astype(F32)
        h = h * h
        return squares + h[:, :128] + h[:, 128:]

    squares = lax.fori_loop(0, 8, mixer_step, jnp.zeros((BLK, 128), F32))
    scale = lax.rsqrt(jnp.sum(squares, axis=1, keepdims=True) * (1.0 / 2048.0) + EPS)
    ring(1)

    def norm_step(n, _):
        nb[:, wide(n)] = (hid[:, wide(n)].astype(F32) * scale * ng_ref[:, wide(n)]).astype(BF16)
        return 0

    lax.fori_loop(0, 8, norm_step, 0)

    xcopies = []
    for j in range(3):

        def pick_step(n, _):
            xs[j, :, :, wide(n)] = dot(wt[j], nb[:, wide(n)]).astype(BF16).reshape(16, 16, 256)
            return 0

        for part in range(PARTS):
            lax.fori_loop(part * 8 // PARTS, (part + 1) * 8 // PARTS, pick_step, 0)
            cols = pl.ds(part * 2048 // PARTS, 2048 // PARTS)
            for i, other in enumerate(partners):
                xcopies.append(go(remote(
                    xs.at[j, other, :, cols], xr.at[j, sp, :, cols], xsend.at[j, part, i], xrecv.at[j, part, i], (other, tp)
                )))
        xr[j, sp] = xs[j, sp]
        ring(1)

    c_sg.wait()
    c_su.wait()

    def shared_step(n, _):
        a = dot(nb[...], sg[:, wide(n)])
        smid[:, wide(n)] = (jax.nn.silu(a) * dot(nb[...], su[:, wide(n)])).astype(BF16)
        return 0

    lax.fori_loop(0, 2, shared_step, 0)
    ring(1)
    c_sd.wait()

    def shared_out(n, _):
        acc[:, wide(n)] = dot(smid[...], sd[wide(n), :], nt) + hid[:, wide(n)].astype(F32)
        return 0

    lax.fori_loop(0, 8, shared_out, 0)
    ring(len(events) - 12)

    def opened(j, n):
        at_n = pl.ds(pl.multiple_of(n * 128, 128), 128)
        rows = xr[j].reshape(BLK, 2048)
        h = dot(rows, jnp.concatenate([gateb[at_n, :], upb[at_n, :]], axis=0), nt)
        mid[:, at_n] = (jax.nn.silu(h[:, :128]) * h[:, 128:]).astype(BF16)

    def landed(offsets, pieces):
        for o in offsets:
            for p in pieces:
                across(o, p, 1 - c).wait_recv()

    for i in range(15 * PARTS):
        xcopies[i].wait_recv()

    def near(i, _):
        opened(0, (z + i + 6) % 8)
        return 0

    def third(i, _):
        opened(0, (z + 3 + 2 * i) % 8)
        return 0

    landed((0, 1, 2, 6, 7), range(4))
    lax.fori_loop(0, 5, near, 0)
    ring(6)
    landed((3, 5), range(4))
    lax.fori_loop(0, 2, third, 0)
    ring(4)
    landed((4,), range(4))
    opened(0, (z + 4) % 8)
    ring(2)
    landed(range(8), (4, 5))

    ycopies = []
    for j in range(3):
        if j > 0:
            for i in range(15 * PARTS):
                xcopies[j * 15 * PARTS + i].wait_recv()

            def up_step(n, _):
                opened(j, n)
                return 0

            lax.fori_loop(0, 8, up_step, 0)

        def down_step(n, _):
            yb[j, :, :, wide(n)] = dot(mid[...], downb[:, wide(n)]).astype(BF16).reshape(16, 16, 256)
            return 0

        for part in range(PARTS):
            lax.fori_loop(part * 8 // PARTS, (part + 1) * 8 // PARTS, down_step, 0)
            cols = pl.ds(part * 2048 // PARTS, 2048 // PARTS)
            for i, other in enumerate(partners):
                ycopies.append(go(remote(
                    yb.at[j, other, :, cols], yr.at[j, sp, :, cols], ysend.at[j, part, i], yrecv.at[j, part, i], (other, tp)
                )))
        yr[j, sp] = yb[j, sp]

    for j in range(3):
        def sum_step(n, _):
            back = yr[j, :, :, wide(n)].reshape(BLK, 256)
            sums = acc[:, wide(n)] + (dot(wt[3 + j], back) + dot(wt[6 + j], back))
            if j < 2:
                acc[:, wide(n)] = sums
            else:
                out_ref[:, wide(n)] = sums.astype(BF16)
            return 0

        for part in range(PARTS):
            for i in range(15):
                ycopies[(j * PARTS + part) * 15 + i].wait_recv()
            lax.fori_loop(part * 8 // PARTS, (part + 1) * 8 // PARTS, sum_step, 0)

    for cp in started + flying[0] + flying[1]:
        cp.wait_send()
    for off in range(1, 16):
        remote(pb.at[0], rb.at[0], tsend.at[off], trecv.at[off], (sp, sibling)).wait_send()


FIRST = 3
AFTER_GATED = 2


def on_device(
    query_rows, key_rows, value_rows, gate_rows, log_decay, residual, head_gain, out_weight, norm_gain,
    expert_ids, route_weights, expert_gate, expert_up, expert_down, shared_gate, shared_up, shared_down,
):
    anywhere = pl.BlockSpec(memory_space=pl.ANY)
    inside = pl.BlockSpec(memory_space=pltpu.VMEM)
    dma = pltpu.SemaphoreType.DMA
    vm = pltpu.VMEM
    return pl.pallas_call(
        layer,
        name="layer",
        out_shape=jax.ShapeDtypeStruct((256, 2048), BF16),
        in_specs=[anywhere] * 4 + [inside, anywhere, inside, anywhere, inside, inside, inside] + [anywhere] * 6,
        out_specs=inside,
        scratch_shapes=[
            *[vm((64, 4096), BF16)] * 4,
            vm((256, 2048), BF16),
            *[vm((2048, 512), BF16)] * 3,
            vm((1024, 128), BF16),
            *[vm((1024, 2048), BF16)] * 4,
            vm((16, 256), F32),
            vm((16, 256, 128), F32),
            vm((16, 64, 64), F32),
            vm((16, 8, 128), F32),
            vm((16, 64, 256), F32),
            vm((40, 128), F32),
            vm((16, 40, 128), F32),
            vm((16, 64, 256), BF16),
            vm((16, 64, 256), BF16),
            vm((256, 1024), BF16),
            vm((256, 2048), BF16),
            vm((256, 2048), BF16),
            *[vm((3, 16, 16, 2048), BF16)] * 4,
            vm((256, 1024), BF16),
            vm((256, 2048), F32),
            vm((9, 256, 256), BF16),
            vm((256, 512), BF16),
            dma((12,)),
            dma((15,)), dma((15,)),
            dma((16,)), dma((16,)),
            dma((16,)), dma((16,)),
            dma((15,)), dma((15,)),
            dma((16,)), dma((16,)),
            dma((2, 4, 6)), dma((2, 4, 6)),
            dma((8, 6)), dma((8, 6)),
            dma((3, PARTS, 15)), dma((3, PARTS, 15)),
            dma((3, PARTS, 15)), dma((3, PARTS, 15)),
        ],
        compiler_params=pltpu.CompilerParams(
            collective_id=0, has_side_effects=True, vmem_limit_bytes=63 * 1024 * 1024
        ),
    )(
        query_rows.T, key_rows.T, value_rows.T, gate_rows.T, log_decay, residual,
        head_gain.reshape(1, 64), out_weight, norm_gain.reshape(1, 2048), expert_ids.T, route_weights.T,
        expert_gate.T, expert_up.T, expert_down.T, shared_gate, shared_up, shared_down,
    )


def solution(mesh):
    placed = (
        P("sp", "tp"),
        P("sp", "tp"),
        P("sp", "tp"),
        P("sp", "tp"),
        P("tp", "sp"),
        P(("sp", "tp"), None),
        P("tp"),
        P(None, "tp"),
        P(),
        P(("sp", "tp"), None),
        P(("sp", "tp"), None),
        P(None, ("sp", "tp")),
        P(None, ("sp", "tp")),
        P(None, ("sp", "tp")),
        P(),
        P(),
        P(),
    )
    return jax.shard_map(
        on_device, mesh=mesh, in_specs=placed, out_specs=P(("sp", "tp"), None), check_vma=False
    )
```

```python
import jax
import jax.numpy as jnp
from jax import lax
from jax.experimental import pallas as pl
from jax.experimental.pallas import tpu as pltpu
from jax.sharding import PartitionSpec as P

HEAD = 64
BLK = 256
EPS = 1e-05
MESH = pl.DeviceIdType.MESH
F32 = jnp.float32
BF16 = jnp.bfloat16
DEPTH = 2
PARTS = 2

FAR = [(2, 2), (1, 2), (2, 1), (2, 3), (3, 2), (1, 1), (3, 3), (1, 3), (3, 1), (2, 0), (0, 2), (1, 0), (0, 1), (3, 0), (0, 3)]


def dot(a, b, dims=((1,), (0,))):
    return lax.dot_general(a, b, (dims, ((), ())), preferred_element_type=F32)


def halves(x):
    high = x.astype(BF16)
    return high, (x - high.astype(F32)).astype(BF16)


def layer(
    q_h, k_h, v_h, g_h, ld_ref, res_h, hg_ref, ow_h, ng_ref, ids_ref, rw_ref,
    gate_h, up_h, down_h, sg_h, su_h, sd_h,
    out_ref,
    q, k, v, g, res, sg, su, sd, ows, owb, gateb, upb, downb,
    cs, cb, cl, lp, inn, st, sr, pb, rb, tr, hid, nb,
    xs, xr, yb, yr, mid, acc, wt, smid,
    lsem, ssend, srecv, tsend, trecv, osend, orecv, wsend, wrecv, vsend, vrecv,
    rsend, rrecv, dsend, drecv, xsend, xrecv, ysend, yrecv,
):
    sp, tp = lax.axis_index("sp"), lax.axis_index("tp")
    y, x = sp // 4, sp % 4
    z, c = tp // 2, tp % 2
    sibling = z * 2 + (1 - c)
    nt, tn = ((1,), (1,)), ((0,), (0,))

    def partner(m):
        dy, dx = m
        dy, dx = jnp.where(c == 0, dy, dx), jnp.where(c == 0, dx, dy)
        return ((y + dy) % 4) * 4 + (x + dx) % 4

    partners = [partner(m) for m in FAR]

    def remote(src, to, here, there, device):
        return pltpu.make_async_remote_copy(src, to, here, there, device_id=device, device_id_type=MESH)

    def local(i, src, to):
        cp = pltpu.make_async_copy(src, to, lsem.at[i])
        cp.start()
        return cp

    def block(ref, size, i):
        return ref.at[pl.ds(pl.multiple_of(i * size, size), size)]

    c_ow = local(0, ow_h, ows)
    c_gate = local(1, gate_h, block(gateb, 64, tp))
    c_up = local(2, up_h, block(upb, 64, tp))
    c_down = local(3, down_h, block(downb, 64, tp))
    c_k = local(4, k_h, k)
    c_v = local(5, v_h, v)
    c_q = local(6, q_h, q)
    c_g = local(7, g_h, g)
    c_res = local(8, res_h, res)
    c_sg = local(9, sg_h, sg)
    c_su = local(10, su_h, su)
    c_sd = local(11, sd_h, sd)

    barrier = pltpu.get_barrier_semaphore()
    for other in partners:
        pl.semaphore_signal(barrier, inc=1, device_id=(other, tp), device_id_type=MESH)
    for step in range(1, 16):
        pl.semaphore_signal(barrier, inc=1, device_id=(sp, (tp + step) % 16), device_id_type=MESH)
    pl.semaphore_wait(barrier, 30)

    def piece(p, j):
        rows = pl.ds(pl.multiple_of(j * 64 + 32 * (p % 2), 32), 32)
        if p < 4:
            return (gateb, upb)[p // 2].at[rows]
        return downb.at[rows, pl.ds(1024 * (p // 2 - 2), 1024)]

    def hop(way, h, p):
        origin = ((z + 8 - h) % 8 if way == 0 else (z + h) % 8) * 2 + c
        to = ((z + 1) % 8 if way == 0 else (z + 7) % 8) * 2 + c
        ref = piece(p, origin)
        return remote(ref, ref, rsend.at[way, h, p], rrecv.at[way, h, p], (sp, to))

    def arrival(way, h, p):
        origin = ((z + 7 - h) % 8 if way == 0 else (z + h + 1) % 8) * 2 + c
        ref = piece(p, origin)
        return remote(ref, ref, rsend.at[way, h, p], rrecv.at[way, h, p], (sp, sibling))

    def across(o, p, core):
        ref = piece(p, ((z + o) % 8) * 2 + core)
        return remote(ref, ref, dsend.at[o, p], drecv.at[o, p], (sp, sibling))

    flying = {0: [], 1: []}
    depth = [DEPTH]
    started = []

    def go(cp):
        cp.start()
        started.append(cp)
        return cp

    def send(way, h, p):
        if len(flying[way]) >= depth[0]:
            flying[way].pop(0).wait_send()
        cp = hop(way, h, p)
        cp.start()
        flying[way].append(cp)

    def event(h, p):
        for way in (0, 1):
            last = p % 2 == way
            if h == 0:
                send(way, 0, p)
                continue
            if h == 4 and not last:
                continue
            arrival(way, h - 1, p).wait_recv()
            if h < 3 or (h == 3 and last):
                send(way, h, p)
            go(across((8 - h) % 8 if way == 0 else h, p, c))
        if h == 0:
            go(across(0, p, c))

    events = [(h, p) for h in range(3) for p in range(4)]
    for first, count, more in (
        (4, 2, [(3, p) for p in range(4)]),
        (None, 0, [(1, 4), (1, 5), (0, 6), (0, 7)] + [(4, p) for p in range(4)]),
        (None, 0, [(2, 4), (2, 5), (1, 6), (1, 7), (3, 4), (3, 5), (2, 6), (2, 7)]),
        (None, 0, [(4, 4), (4, 5), (3, 6), (3, 7), (4, 6), (4, 7)]),
    ):
        events += [(0, first + i) for i in range(count)] + more
    total_events = len(events)

    def ring_to(n):
        ring(n - (total_events - len(events)))

    def ring(n):
        for _ in range(n):
            if events:
                event(*events.pop(0))

    def slice_of(core):
        return pl.ds(pl.multiple_of(sp * 64 + core * 32, 32), 32)

    def columns_of(j):
        return pl.ds(pl.multiple_of(j * 128, 128), 128)

    c_ow.wait()
    for step in range(1, 16):
        other = (tp + step) % 16
        go(remote(
            ows.at[slice_of((c + step) % 2), :], owb.at[slice_of((c + step) % 2), columns_of(tp)],
            osend.at[step], orecv.at[step], (sp, other),
        ))
    owb[slice_of(c), columns_of(tp)] = ows[slice_of(c), :]
    c_gate.wait()
    c_up.wait()
    c_down.wait()
    ring(FIRST)

    ri = lax.broadcasted_iota(jnp.int32, (BLK, BLK), 0)
    ci = lax.broadcasted_iota(jnp.int32, (BLK, BLK), 1)
    upper = (ri <= ci).astype(F32).astype(BF16)
    lower = (ri >= ci).astype(F32).astype(BF16)
    for b in range(16):
        cs[b : b + 1, :] = ld_ref[0:1, b * BLK : b * BLK + BLK]
    ld = cs[...]
    d0 = ld.astype(BF16)
    left = ld - d0.astype(F32)
    d1 = left.astype(BF16)
    d2 = (left - d1.astype(F32)).astype(BF16)
    cs[...] = dot(d0, upper) + (dot(d1, upper) + dot(d2, upper))
    cols = dot(lower, d0, nt) + (dot(lower, d1, nt) + dot(lower, d2, nt))
    for b in range(16):
        cb[b] = jnp.broadcast_to(cols[:, b : b + 1], (BLK, 128))

    c_k.wait()
    c_v.wait()

    def at(b):
        return pl.ds(pl.multiple_of(b * BLK, BLK), BLK)

    def state_step(b, carry):
        state, total = carry
        cl[b] = state
        lp[b] = jnp.broadcast_to(total, (8, 128))
        end = cb[b, BLK - 1 : BLK, :]
        wide = jnp.concatenate([end, end], axis=1)
        kd = k[:, at(b)].astype(F32) * (jnp.exp(wide - cs[pl.ds(b, 1), :]) * 0.125)
        high, low = halves(kd)
        vb = v[:, at(b)]
        state = state * jnp.exp(end[:, :HEAD]) + (dot(vb, high, nt) + dot(vb, low, nt))
        return state, total + end

    state, total = lax.fori_loop(
        0, 16, state_step, (jnp.zeros((HEAD, HEAD), F32), jnp.zeros((1, 128), F32)), unroll=2
    )
    st[0:32] = jnp.concatenate([state[:32], state[32:]], axis=1)
    st[32:40] = jnp.broadcast_to(total, (8, 128))
    scopies = []
    for i, other in enumerate(partners):
        scopies.append(go(remote(st, sr.at[sp], ssend.at[i], srecv.at[i], (other, tp))))
    sr[sp] = st[...]

    for step in range(1, 16):
        remote(
            ows.at[slice_of(c), :], owb.at[slice_of(c), columns_of(tp)], osend.at[step], orecv.at[step], (sp, sibling)
        ).wait_recv()

    def part_of(s, a):
        return owb.at[pl.ds(pl.multiple_of(s * 64 + c * 32 + a * 16, 16), 16)]

    def placed(a, along, other):
        return partner((along % 4, other % 4) if a == 0 else (other % 4, along % 4))

    routes = [(2, 0), (1, 0), (3, 0)]
    for d, _ in routes:
        for a in (0, 1):
            go(remote(part_of(sp, a), part_of(sp, a), wsend.at[a, d, 0], wrecv.at[a, d, 0], (placed(a, d, 0), tp)))

    def pass_on(a, d0):
        ref = part_of(placed(a, 4 - d0, 0), a) if d0 else part_of(sp, a)
        for d in (2, 1, 3):
            go(remote(ref, ref, wsend.at[a, d0, d], wrecv.at[a, d0, d], (placed(a, 0, d), tp)))
        go(remote(ref, ref, vsend.at[a, d0, 0], vrecv.at[a, d0, 0], (sp, sibling)))

    for a in (0, 1):
        pass_on(a, 0)
    ring(1)
    c_q.wait()

    def inner_step(b, _):
        scores = dot(k[:, at(b)], q[:, at(b)], tn)
        spread = cs[pl.ds(b, 1), :] - jnp.concatenate([cb[b], cb[b]], axis=1)
        damp = jnp.exp(jnp.where(ri <= ci, spread, -jnp.inf))
        inn[b] = dot(v[:, at(b)], (scores * 0.125 * damp).astype(BF16))
        return 0

    for part in range(2):
        lax.fori_loop(part * 8, part * 8 + 8, inner_step, 0, unroll=2)
        ring(1)
    for d0, _ in routes:
        for a in (0, 1):
            ref = part_of(placed(a, 4 - d0, 0), a)
            remote(ref, ref, wsend.at[a, d0, 0], wrecv.at[a, d0, 0], (sp, sibling)).wait_recv()
            pass_on(a, d0)

    e_i = lax.broadcasted_iota(jnp.int32, (16, BLK), 0)
    first, second = ids_ref[0:1, :] == e_i, ids_ref[1:2, :] == e_i
    named = jnp.where(first | second, 1.0, 0.0)
    before = dot(named.astype(BF16), (ri < ci).astype(F32).astype(BF16))
    code = jnp.where(named > 0, before, -1.0)
    share = jnp.where(first, rw_ref[0:1, :], 0.0) + jnp.where(second, rw_ref[1:2, :], 0.0)
    codes = jnp.broadcast_to(code[:, None, :], (16, 16, BLK)).reshape(BLK, BLK)
    shares = jnp.broadcast_to(share[:, None, :], (16, 16, BLK)).reshape(BLK, BLK)
    slot = (ri % 16).astype(F32)
    for j in range(3):
        chosen = codes == slot + 16.0 * j
        wt[j] = jnp.where(chosen, 1.0, 0.0).astype(BF16)
        high, low = halves(jnp.where(chosen, shares, 0.0).T)
        wt[3 + j] = high
        wt[6 + j] = low

    gain = jnp.broadcast_to(hg_ref[...], (BLK, HEAD)).T
    c_g.wait()
    for cp in scopies:
        cp.wait_recv()

    def entering(j, inc):
        have = sr[j]
        return jnp.where(j < sp, inc * jnp.exp(have[32:33]) + have[:32], inc)

    packed = lax.fori_loop(0, 16, entering, jnp.zeros((32, 128), F32))
    inc = jnp.concatenate([packed[:, :HEAD], packed[:, HEAD:]], axis=0)

    def gated(i):
        off = (8 + i) % 16
        b = (tp + off) % 16
        high, low = halves(cl[b] + inc * jnp.exp(lp[b, 0:1, :HEAD]))
        qb = q[:, at(b)]
        kept = inn[b] + (dot(high, qb) + dot(low, qb)) * jnp.exp(cs[pl.ds(b, 1), :])
        kept = kept - jnp.mean(kept, axis=0, keepdims=True)
        kept = kept * lax.rsqrt(jnp.mean(kept * kept, axis=0, keepdims=True) + EPS)
        pb[b] = (kept * gain * jax.nn.silu(g[:, at(b)].astype(F32))).astype(BF16)
        return off, b

    def gated_step(i, _):
        pairs = [gated(2 * i), gated(2 * i + 1)]
        for off, b in pairs:

            @pl.when(off != 0)
            def _():
                remote(pb.at[b], rb.at[tp], tsend.at[off], trecv.at[off], (sp, b)).start()

            @pl.when(off == 0)
            def _():
                rb[tp] = pb[b]

        return 0

    lax.fori_loop(0, 8, gated_step, 0)
    ring(AFTER_GATED)

    for d0 in (0, 2, 1, 3):
        for a in (0, 1):
            for d in (2, 1, 3):
                ref = part_of(placed(a, 4 - d0, 4 - d), a)
                remote(ref, ref, wsend.at[a, d0, d], wrecv.at[a, d0, d], (sp, sibling)).wait_recv()
                go(remote(ref, ref, vsend.at[a, d0, d], vrecv.at[a, d0, d], (sp, sibling)))

    for off in range(1, 16):
        remote(pb.at[0], rb.at[0], tsend.at[off], trecv.at[off], (sp, sibling)).wait_recv()
    for i in range(8):
        both = jnp.concatenate([rb[2 * i], rb[2 * i + 1]], axis=0)
        tr[:, 128 * i : 128 * i + 128] = both.astype(F32).T.astype(BF16)
    ring(1)
    for d0 in range(4):
        for a in (0, 1):
            for d in range(4):
                remote(part_of(sp, a), part_of(sp, a), vsend.at[a, d0, d], vrecv.at[a, d0, d], (sp, sibling)).wait_recv()
    c_res.wait()

    def wide(n):
        return pl.ds(pl.multiple_of(n * 256, 256), 256)

    def mixer_step(n, squares):
        h = (res[:, wide(n)].astype(F32) + dot(tr[...], owb[:, wide(n)])).astype(BF16)
        hid[:, wide(n)] = h
        h = h.astype(F32)
        h = h * h
        return squares + h[:, :128] + h[:, 128:]

    squares = lax.fori_loop(0, 8, mixer_step, jnp.zeros((BLK, 128), F32))
    scale = lax.rsqrt(jnp.sum(squares, axis=1, keepdims=True) * (1.0 / 2048.0) + EPS)
    ring(1)

    def norm_step(n, _):
        nb[:, wide(n)] = (hid[:, wide(n)].astype(F32) * scale * ng_ref[:, wide(n)]).astype(BF16)
        return 0

    lax.fori_loop(0, 8, norm_step, 0)

    xcopies = []
    for j in range(3):

        def pick_step(n, _):
            xs[j, :, :, wide(n)] = dot(wt[j], nb[:, wide(n)]).astype(BF16).reshape(16, 16, 256)
            return 0

        for part in range(PARTS):
            lax.fori_loop(part * 8 // PARTS, (part + 1) * 8 // PARTS, pick_step, 0)
            cols = pl.ds(part * 2048 // PARTS, 2048 // PARTS)
            for i, other in enumerate(partners):
                xcopies.append(go(remote(
                    xs.at[j, other, :, cols], xr.at[j, sp, :, cols], xsend.at[j, part, i], xrecv.at[j, part, i], (other, tp)
                )))
        xr[j, sp] = xs[j, sp]
        ring(1)

    c_sg.wait()
    c_su.wait()

    def shared_step(n, _):
        a = dot(nb[...], sg[:, wide(n)])
        smid[:, wide(n)] = (jax.nn.silu(a) * dot(nb[...], su[:, wide(n)])).astype(BF16)
        return 0

    lax.fori_loop(0, 2, shared_step, 0)
    ring(1)
    c_sd.wait()

    def shared_out(n, _):
        acc[:, wide(n)] = dot(smid[...], sd[wide(n), :], nt) + hid[:, wide(n)].astype(F32)
        return 0

    lax.fori_loop(0, 8, shared_out, 0)
    depth[0] = 8
    ring_to(14)

    def opened(j, n):
        at_n = pl.ds(pl.multiple_of(n * 128, 128), 128)
        rows = xr[j].reshape(BLK, 2048)
        h = dot(rows, jnp.concatenate([gateb[at_n, :], upb[at_n, :]], axis=0), nt)
        mid[j, :, at_n] = (jax.nn.silu(h[:, :128]) * h[:, 128:]).astype(BF16)

    def landed(offsets, pieces):
        for o in offsets:
            for p in pieces:
                across(o, p, 1 - c).wait_recv()

    def came(j):
        for i in range(15 * PARTS):
            xcopies[j * 15 * PARTS + i].wait_recv()

    def opened_some(j, begin, end):
        def up_step(n, _):
            opened(j, n)
            return 0

        lax.fori_loop(begin, end, up_step, 0)

    def near(i, _):
        opened(0, (z + i + 6) % 8)
        return 0

    def third(i, _):
        opened(0, (z + 3 + 2 * i) % 8)
        return 0

    ycopies = {}

    def closed(j, part):
        def down_step(n, _):
            yb[j, :, :, wide(n)] = dot(mid[j], downb[:, wide(n)]).astype(BF16).reshape(16, 16, 256)
            return 0

        lax.fori_loop(part * 4, part * 4 + 4, down_step, 0)
        cols = pl.ds(part * 1024, 1024)
        ycopies[j, part] = [
            go(remote(
                yb.at[j, other, :, cols], yr.at[j, sp, :, cols], ysend.at[j, part, i], yrecv.at[j, part, i], (other, tp)
            ))
            for i, other in enumerate(partners)
        ]
        yr[j, sp, :, cols] = yb[j, sp, :, cols]

    came(0)
    landed((0, 1, 2, 6, 7), range(4))
    lax.fori_loop(0, 5, near, 0)
    ring_to(18)
    landed((3, 5), range(4))
    lax.fori_loop(0, 2, third, 0)
    ring_to(26)
    landed((4,), range(4))
    opened(0, (z + 4) % 8)
    ring_to(30)
    came(1)
    for begin, end, events_done in ((0, 3, 32), (3, 6, 34), (6, 8, 36)):
        opened_some(1, begin, end)
        ring_to(events_done)
    landed(range(8), (4, 5))
    closed(0, 0)
    closed(1, 0)
    ring_to(38)
    came(2)
    opened_some(2, 0, 8)
    closed(2, 0)
    ring_to(40)
    landed(range(8), (6, 7))
    for j in range(3):
        closed(j, 1)

    for cp in started[: -15 * 6] + flying[0] + flying[1]:
        cp.wait_send()
    for part in range(2):
        for j in range(3):

            def sum_step(n, _):
                back = yr[j, :, :, wide(n)].reshape(BLK, 256)
                sums = acc[:, wide(n)] + (dot(wt[3 + j], back) + dot(wt[6 + j], back))
                if j < 2:
                    acc[:, wide(n)] = sums
                else:
                    out_ref[:, wide(n)] = sums.astype(BF16)
                return 0

            for cp in ycopies[j, part]:
                cp.wait_recv()
            lax.fori_loop(part * 4, part * 4 + 4, sum_step, 0)

    for cp in started[-15 * 6 :]:
        cp.wait_send()
    for off in range(1, 16):
        remote(pb.at[0], rb.at[0], tsend.at[off], trecv.at[off], (sp, sibling)).wait_send()


FIRST = 2
AFTER_GATED = 1


def on_device(
    query_rows, key_rows, value_rows, gate_rows, log_decay, residual, head_gain, out_weight, norm_gain,
    expert_ids, route_weights, expert_gate, expert_up, expert_down, shared_gate, shared_up, shared_down,
):
    anywhere = pl.BlockSpec(memory_space=pl.ANY)
    inside = pl.BlockSpec(memory_space=pltpu.VMEM)
    dma = pltpu.SemaphoreType.DMA
    vm = pltpu.VMEM
    return pl.pallas_call(
        layer,
        name="layer",
        out_shape=jax.ShapeDtypeStruct((256, 2048), BF16),
        in_specs=[anywhere] * 4 + [inside, anywhere, inside, anywhere, inside, inside, inside] + [anywhere] * 6,
        out_specs=inside,
        scratch_shapes=[
            *[vm((64, 4096), BF16)] * 4,
            vm((256, 2048), BF16),
            *[vm((2048, 512), BF16)] * 3,
            vm((1024, 128), BF16),
            *[vm((1024, 2048), BF16)] * 4,
            vm((16, 256), F32),
            vm((16, 256, 128), F32),
            vm((16, 64, 64), F32),
            vm((16, 8, 128), F32),
            vm((16, 64, 256), F32),
            vm((40, 128), F32),
            vm((16, 40, 128), F32),
            vm((16, 64, 256), BF16),
            vm((16, 64, 256), BF16),
            vm((256, 1024), BF16),
            vm((256, 2048), BF16),
            vm((256, 2048), BF16),
            *[vm((3, 16, 16, 2048), BF16)] * 4,
            vm((3, 256, 1024), BF16),
            vm((256, 2048), F32),
            vm((9, 256, 256), BF16),
            vm((256, 512), BF16),
            dma((12,)),
            dma((15,)), dma((15,)),
            dma((16,)), dma((16,)),
            dma((16,)), dma((16,)),
            dma((2, 4, 4)), dma((2, 4, 4)),
            dma((2, 4, 4)), dma((2, 4, 4)),
            dma((2, 4, 8)), dma((2, 4, 8)),
            dma((8, 8)), dma((8, 8)),
            dma((3, PARTS, 15)), dma((3, PARTS, 15)),
            dma((3, PARTS, 15)), dma((3, PARTS, 15)),
        ],
        compiler_params=pltpu.CompilerParams(
            collective_id=0, has_side_effects=True, vmem_limit_bytes=63 * 1024 * 1024
        ),
    )(
        query_rows.T, key_rows.T, value_rows.T, gate_rows.T, log_decay, residual,
        head_gain.reshape(1, 64), out_weight, norm_gain.reshape(1, 2048), expert_ids.T, route_weights.T,
        expert_gate.T, expert_up.T, expert_down.T, shared_gate, shared_up, shared_down,
    )


def solution(mesh):
    placed = (
        P("sp", "tp"),
        P("sp", "tp"),
        P("sp", "tp"),
        P("sp", "tp"),
        P("tp", "sp"),
        P(("sp", "tp"), None),
        P("tp"),
        P(None, "tp"),
        P(),
        P(("sp", "tp"), None),
        P(("sp", "tp"), None),
        P(None, ("sp", "tp")),
        P(None, ("sp", "tp")),
        P(None, ("sp", "tp")),
        P(),
        P(),
        P(),
    )
    return jax.shard_map(
        on_device, mesh=mesh, in_specs=placed, out_specs=P(("sp", "tp"), None), check_vma=False
    )
```
